256 devices in a mesh: sp: 64 (over z, y, core), tp: 4 (over x).
Axes of the slice: x: 4, y: 4, z: 8, core: 2. Of those that a mesh axis runs over, the one named last changes fastest.
Arguments:
- tokens: bfloat16 [16384, 2048], P('sp', 'tp'), may hold values from -19 to 250
- in_gain: bfloat16 [2048], replicated, may hold values from 0.099609375 to 1.8984375
- w_glu_value: bfloat16 [2048, 512], P(None, 'tp'), may hold values from -0.125 to 0.125
- w_glu_gate: bfloat16 [2048, 512], P(None, 'tp'), may hold values from -0.125 to 0.125
- w_query: bfloat16 [2048, 1024], P(None, 'tp'), may hold values from -1 to 1
- w_key: bfloat16 [2048, 512], P(None, 'tp'), may hold values from -1 to 1
- w_value: bfloat16 [2048, 512], P(None, 'tp'), may hold values from -0.125 to 0.125
- w_gate_conv: bfloat16 [2048, 512], P(None, 'tp'), may hold values from -0.125 to 0.125
- w_gate_attn: bfloat16 [2048, 1024], P(None, 'tp'), may hold values from -0.125 to 0.125
- conv_weight: bfloat16 [31, 512], P(None, 'tp'), may hold values from -4.6 to 4.6
- conv_gain: float32 [512], P('tp'), may hold values from 0.1 to 1.9
- lam: float32 [8], P('tp'), may hold values from 0.3 to 0.8
- head_gain: float32 [128], replicated, may hold values from 0.1 to 1.9
- out_conv: bfloat16 [512, 2048], P('tp'), may hold values from -0.15625 to 0.15625
- out_attn: bfloat16 [1024, 2048], P('tp'), may hold values from -0.15625 to 0.15625
Outputs:
- mixed: bfloat16 [16384, 2048], P(('sp', 'tp'))
The draws below stay inside these ranges and needn't reach their ends.
All inputs are finite; a program needn't handle non-finite values.
Results may differ from the reference program's by a relative error of at most 0.017.
The reference program's roundings to bfloat16 on the way count: a program that leaves them out, or rounds other values in their place, can miss the bound.
Values may be sent and summed in bfloat16 or wider, within the bound.
No kernel may reach another device: no remote copies, remote signals or barrier semaphores. Data moves between devices by JAX's collectives and lax.ppermute only.
A program may use at most 128 MiB of HBM per device.

```python
import math
import jax
import jax.numpy as jnp
from jax import lax

D = 2048
CONV = 512
HEADS = 8
KV_HEADS = 4
QK = 64
VDIM = 128
WIDTH = 31
TOKENS = 16384
N_TP = 4


def draw_tokens(key, part):
    k_base = jax.random.fold_in(jax.random.fold_in(key, 11), 0)
    values = jnp.clip(jax.random.normal(k_base, (TOKENS, D), jnp.float32), -6.0, 6.0)
    return values.astype(jnp.bfloat16)


def draw_w_query(key, part):
    values = jnp.clip(jax.random.normal(jax.random.fold_in(key, 21), (D, HEADS * 2 * QK), jnp.float32), -6.0, 6.0)
    values = values * (1.3 / jnp.sqrt(jnp.float32(D)))
    return values.astype(jnp.bfloat16)


def draw_w_key(key, part):
    values = jnp.clip(jax.random.normal(jax.random.fold_in(key, 22), (D, KV_HEADS * 2 * QK), jnp.float32), -6.0, 6.0)
    values = values * (1.3 / jnp.sqrt(jnp.float32(D)))
    return values.astype(jnp.bfloat16)


def draw_conv_weight(key, part):
    k_base, k_rough = jax.random.split(jax.random.fold_in(key, 31), 2)
    position = jnp.arange(CONV, dtype=jnp.float32) / CONV
    trend = 3.0 ** (position - 0.5)
    rough = jnp.exp(jax.random.uniform(k_rough, (CONV,), jnp.float32, -0.7, 0.7))
    values = jnp.clip(jax.random.normal(k_base, (WIDTH, CONV), jnp.float32), -4.0, 4.0)
    values = values / jnp.sqrt(jnp.float32(WIDTH)) * (trend * rough)[None, :]
    return values.astype(jnp.bfloat16)


def shard_levels(stream_key, shape, cuts, smallest, largest):
    gain, own = 1.0, jax.random.fold_in(stream_key, 6)
    for dim, parts in cuts:
        heights = jnp.exp(jax.random.uniform(jax.random.fold_in(own, dim), (parts,), jnp.float32, smallest / len(cuts), largest / len(cuts)))
        gain = gain * jnp.repeat(heights, shape[dim] // parts).reshape([-1 if axis == dim else 1 for axis in range(len(shape))])
    return gain


def gaussian(rng, shape, deviation, reach, cuts=(), kind=jnp.bfloat16):
    level = shard_levels(rng, shape, cuts, -0.22, 0.18) if cuts else 1.0
    entries = jax.random.normal(rng, shape, jnp.float32) * deviation * level
    return jnp.minimum(jnp.maximum(entries, -reach), reach).astype(kind)


def setup_inputs(seed: int = 0) -> dict:
    streams_of = jax.random.split(jax.random.key(seed), 16)
    return {
        "tokens": draw_tokens(jax.random.fold_in(streams_of[15], 71), 0),
        "in_gain": jnp.clip(1.0 + 0.18 * jax.random.normal(streams_of[1], (D,), jnp.float32), 0.099609375, 1.8984375).astype(jnp.bfloat16),
        "w_glu_value": gaussian(streams_of[2], (D, CONV), D ** -0.5, 0.125, ((1, 4),)),
        "w_glu_gate": gaussian(streams_of[3], (D, CONV), D ** -0.5, 0.125, ((1, 4),)),
        "w_query": draw_w_query(jax.random.fold_in(streams_of[15], 71), 0),
        "w_key": draw_w_key(jax.random.fold_in(streams_of[15], 71), 0),
        "w_value": gaussian(streams_of[6], (D, KV_HEADS * VDIM), D ** -0.5, 0.125, ((1, 4),)),
        "w_gate_conv": gaussian(streams_of[7], (D, CONV), D ** -0.5, 0.125, ((1, 4),)),
        "w_gate_attn": gaussian(streams_of[8], (D, HEADS * VDIM), D ** -0.5, 0.125, ((1, 4),)),
        "conv_weight": draw_conv_weight(jax.random.fold_in(streams_of[15], 71), 0),
        "conv_gain": jnp.clip(1.0 + 0.18 * jax.random.normal(streams_of[10], (CONV,), jnp.float32), 0.1, 1.9),
        "lam": jnp.clip(0.3 + 0.5 * jax.random.uniform(streams_of[11], (HEADS,), jnp.float32) ** shard_levels(streams_of[11], (HEADS,), ((0, 4),), -0.2, 0.2), 0.3, 0.8),
        "head_gain": jnp.clip(1.0 + 0.18 * jax.random.normal(streams_of[12], (VDIM,), jnp.float32), 0.1, 1.9),
        "out_conv": gaussian(streams_of[13], (CONV, D), (CONV + HEADS * VDIM) ** -0.5, 0.15625, ((0, 4),)),
        "out_attn": gaussian(streams_of[14], (HEADS * VDIM, D), (CONV + HEADS * VDIM) ** -0.5, 0.15625, ((0, 4),)),
    }


EPSILON = 1e-06
NEG_BIG = -1e+30
HEAD_SCALE = 0.8

def attend_head(query_head, key_head, value_head, lam_head, head_gain):
    block_rows = math.gcd(TOKENS, 512)
    blocks = TOKENS // block_rows
    scale_factor = 1.0 / math.sqrt(QK)

    def one_block(index):
        query_block = lax.dynamic_slice_in_dim(query_head, index * block_rows, block_rows, 0).astype(jnp.float32)
        query_pos = index * block_rows + jnp.arange(block_rows, dtype=jnp.int32)

        def visit(other, running):
            maxima, totals, summed = running
            key_block = lax.dynamic_slice_in_dim(key_head, other * block_rows, block_rows, 0).astype(jnp.float32)
            value_block = lax.dynamic_slice_in_dim(value_head, other * block_rows, block_rows, 0).astype(jnp.float32)
            scores = jnp.einsum('qcd,kcd->cqk', query_block, key_block) * scale_factor
            key_pos = other * block_rows + jnp.arange(block_rows, dtype=jnp.int32)
            scores = jnp.where(key_pos[None, None, :] <= query_pos[None, :, None], scores, NEG_BIG)
            new_max = jnp.maximum(maxima, lax.optimization_barrier(jnp.max(scores, axis=2)))
            factor = jnp.exp(maxima - new_max)
            expd = jnp.exp(scores - new_max[:, :, None])
            totals = totals * factor + lax.optimization_barrier(jnp.sum(expd, axis=2))
            rounded = lax.optimization_barrier(expd.astype(jnp.bfloat16)).astype(jnp.float32)
            summed = summed * factor[:, :, None] + jnp.einsum('cqk,kv->cqv', rounded, value_block)
            return (new_max, totals, summed)
        start_state = (jnp.full((2, block_rows), NEG_BIG, jnp.float32), jnp.zeros((2, block_rows), jnp.float32), jnp.zeros((2, block_rows, VDIM), jnp.float32))
        maxima, totals, summed = lax.fori_loop(0, index + 1, visit, start_state)
        output = summed[0] / totals[0][:, None] - lam_head * summed[1] / totals[1][:, None]
        normed = output * lax.rsqrt(lax.optimization_barrier(jnp.mean(output * output, axis=1, keepdims=True)) + EPSILON)
        return normed * head_gain[None, :] * HEAD_SCALE
    result = lax.map(one_block, jnp.arange(blocks, dtype=jnp.int32))
    return result.reshape(TOKENS, VDIM)

def reference(tokens, in_gain, w_glu_value, w_glu_gate, w_query, w_key, w_value, w_gate_conv, w_gate_attn, conv_weight, conv_gain, lam, head_gain, out_conv, out_attn):
    widened = tokens.astype(jnp.float32)
    inv_rms = lax.rsqrt(lax.optimization_barrier(jnp.mean(widened * widened, axis=1, keepdims=True)) + EPSILON)
    scaled = (widened * in_gain.astype(jnp.float32)[None, :]).astype(jnp.bfloat16)

    def project(weight):
        return (jnp.dot(scaled, weight, preferred_element_type=jnp.float32) * inv_rms).astype(jnp.bfloat16)
    glu_value = project(w_glu_value)
    glu_gate = project(w_glu_gate)
    query = project(w_query)
    key = project(w_key)
    value = project(w_value)
    gate_conv = project(w_gate_conv)
    gate_attn = project(w_gate_attn)
    glued = (glu_value.astype(jnp.float32) * jax.nn.sigmoid(glu_gate.astype(jnp.float32))).astype(jnp.bfloat16)
    padded = jnp.pad(glued.astype(jnp.float32), ((WIDTH - 1, 0), (0, 0)))
    taps = conv_weight.astype(jnp.float32)
    conv = jnp.zeros((TOKENS, CONV), jnp.float32)
    for offset in range(WIDTH):
        conv = conv + padded[offset:offset + TOKENS] * taps[offset][None, :]
    channel_ms = lax.optimization_barrier(jnp.mean(conv * conv, axis=1, keepdims=True))
    conv_normed = conv * lax.rsqrt(channel_ms + EPSILON) * conv_gain[None, :]
    y_conv = (jax.nn.silu(conv_normed) * jax.nn.silu(gate_conv.astype(jnp.float32))).astype(jnp.bfloat16)
    group = HEADS // KV_HEADS
    query_heads = jnp.transpose(query.reshape(TOKENS, HEADS, 2, QK), (1, 0, 2, 3))
    key_heads = jnp.transpose(key.reshape(TOKENS, KV_HEADS, 2, QK), (1, 0, 2, 3))
    value_heads = jnp.transpose(value.reshape(TOKENS, KV_HEADS, VDIM), (1, 0, 2))

    def per_head(head):
        shared = head // group
        return attend_head(query_heads[head], key_heads[shared], value_heads[shared], lam[head], head_gain)
    heads_out = lax.map(per_head, jnp.arange(HEADS, dtype=jnp.int32))
    attn_normed = jnp.transpose(heads_out, (1, 0, 2)).reshape(TOKENS, HEADS * VDIM)
    y_attn = (attn_normed * jax.nn.silu(gate_attn.astype(jnp.float32))).astype(jnp.bfloat16)
    conv_block = CONV // N_TP
    attn_block = HEADS * VDIM // N_TP
    mixed = jnp.zeros((TOKENS, D), jnp.float32)
    for member in range(N_TP):
        partial_value = jnp.dot(y_conv[:, member * conv_block:(member + 1) * conv_block], out_conv[member * conv_block:(member + 1) * conv_block], preferred_element_type=jnp.float32)
        partial_value = partial_value + jnp.dot(y_attn[:, member * attn_block:(member + 1) * attn_block], out_attn[member * attn_block:(member + 1) * attn_block], preferred_element_type=jnp.float32)
        mixed = mixed + lax.optimization_barrier(partial_value.astype(jnp.bfloat16)).astype(jnp.float32)
    return mixed.astype(jnp.bfloat16)
```

```python
import functools

import jax
import jax.numpy as jnp
from jax import lax
from jax.experimental import pallas as pl
from jax.experimental.pallas import tpu as pltpu
from jax.sharding import PartitionSpec as P

D = 2048
CONV = 512
QK = 64
VDIM = 128
WIDTH = 31
ROWS = 256
ACC = VDIM + 16
MSG = 4 * VDIM + 16

EPSILON = 1e-06
NEG_BIG = -1e30
HEAD_SCALE = 0.8


F32 = jnp.float32
BF16 = jnp.bfloat16
VM = pl.BlockSpec(memory_space=pltpu.VMEM)
SM = pl.BlockSpec(memory_space=pltpu.SMEM)
ANY = pl.BlockSpec(memory_space=pl.ANY)
BIG = pltpu.CompilerParams(vmem_limit_bytes=56 * 1024 * 1024)
SHIFTS = (1, -1, 2)


def place(s):
    return s // 8, (s // 2) % 4, s % 2


def along_sp(x, move):
    pairs = []
    for s in range(64):
        z, y, c = place(s)
        z, y, c = move(z, y, c)
        pairs.append((s, z * 8 + y * 2 + c))
    return lax.ppermute(x, "sp", pairs)


def z_shift(x, by):
    return along_sp(x, lambda z, y, c: ((z + by) % 8, y, c))


def y_shift(x, by):
    return along_sp(x, lambda z, y, c: (z, (y + by) % 4, c))


def core_swap(x):
    return along_sp(x, lambda z, y, c: (z, y, 1 - c))


def tp_shift(x, by):
    return lax.ppermute(x, "tp", [(i, (i + by) % 4) for i in range(4)])


def dot(a, b):
    return jnp.dot(a, b, preferred_element_type=F32)


def project_kernel(t0, t1, t2, t3, gain, wgv, wgg, wq, wk, wv, wgc, wga, qt, kv, glued, tail, gates, scaled):
    x = lax.axis_index("tp")
    squares = jnp.zeros((ROWS, 128), F32)
    for ref, by in zip((t0, t1, t2, t3), (0,) + SHIFTS):
        j = lax.rem(x - by + 4, 4)
        wide = ref[...].astype(F32)
        scaled[j] = (wide * gain[pl.ds(j, 1), :]).astype(BF16)
        sq = wide * wide
        squares += (sq[:, 0:128] + sq[:, 128:256]) + (sq[:, 256:384] + sq[:, 384:512])
    inv = lax.rsqrt(jnp.sum(squares, axis=1, keepdims=True) / D + EPSILON)
    rows = jnp.concatenate([scaled[j] for j in range(4)], axis=1)
    both = dot(rows, jnp.concatenate([wk[...], wv[...]], axis=1)) * inv
    kv[0:256, :] = both[:, 0:128].astype(BF16)
    vt = jnp.transpose(both[:, 128:256]).astype(BF16)
    kv[256:384, :] = vt[:, 0:128]
    kv[384:512, :] = vt[:, 128:256]
    q = dot(rows, wq[...]) * inv
    qt[...] = jnp.transpose(q * (QK ** -0.5)).astype(BF16)
    glu = (dot(rows, jnp.concatenate([wgv[...], wgg[...]], axis=1)) * inv).astype(BF16).astype(F32)
    g = (glu[:, 0:128] * jax.nn.sigmoid(glu[:, 128:256])).astype(BF16)
    glued[...] = g
    tail[...] = g[ROWS - 32 :, :]
    gates[:, 0:128] = (dot(rows, wgc[...]) * inv).astype(BF16)
    gates[:, 128:384] = (dot(rows, wga[...]) * inv).astype(BF16)


def conv_kernel(glued, before, weight, conv, squares, padded):
    padded[0:32, :] = before[...].astype(F32)
    padded[32 : 32 + ROWS, :] = glued[...].astype(F32)
    taps = weight[...].astype(F32)
    total = jnp.zeros((ROWS, 128), F32)
    for j in range(WIDTH):
        total += padded[j + 2 : j + 2 + ROWS, :] * taps[j : j + 1, :]
    conv[...] = total
    squares[...] = jnp.sum(jnp.transpose(total * total), axis=0, keepdims=True)


def gate_kernel(conv, s0, s1, s2, s3, gain, gates, y_conv):
    total = (s0[...] + s1[...]) + (s2[...] + s3[...])
    inv = lax.rsqrt(total / CONV + EPSILON)
    inv = jnp.transpose(jnp.broadcast_to(inv, (128, ROWS)))
    normed = conv[...] * inv * gain[...]
    y_conv[...] = (jax.nn.silu(normed) * jax.nn.silu(gates[:, 0:128].astype(F32))).astype(BF16)


def attend(tiles, kv, slot, queries, maxima, acc, mask=None):
    keys = jnp.concatenate([kv[slot, 0, 0:256, :], kv[slot, 1, 0:256, :]], axis=0)
    values = jnp.concatenate(
        [
            kv[slot, 0, 256:384, :],
            kv[slot, 0, 384:512, :],
            kv[slot, 1, 256:384, :],
            kv[slot, 1, 384:512, :],
        ],
        axis=1,
    )
    values = jnp.concatenate([values, jnp.ones((ACC - VDIM, 512), BF16)], axis=0)
    ahead = dot(keys, queries[tiles[0]])
    for i, t in enumerate(tiles):
        scores = ahead
        if i + 1 < len(tiles):
            ahead = dot(keys, queries[tiles[i + 1]])
        if mask is not None:
            scores = jnp.where(mask, scores, NEG_BIG)
        old = maxima[t]
        new = jnp.maximum(old, jnp.max(scores, axis=0, keepdims=True))
        factor = jnp.exp(old - new)
        expd = jnp.exp(scores - new).astype(BF16)
        acc[t] = acc[t] * factor + dot(values, expd)
        maxima[t] = new


def attention_kernel(*refs):
    q_refs, kv_own, kv_other, outs = refs[0:4], refs[4:13], refs[13:22], refs[22:26]
    kv, queries, maxima, acc, sems = refs[26:]
    s = lax.axis_index("sp")
    z, y, c = s // 8, lax.rem(s // 2, 4), lax.rem(s, 2)
    copies = []

    def bring(src, dst):
        copy = pltpu.make_async_copy(src, dst, sems.at[len(copies)])
        copy.start()
        copies.append(copy)

    for refs_of, core in ((kv_own, c), (kv_other, 1 - c)):
        for d, r in zip((0, 1, 7, 2, 6, 3, 5), refs_of[0:7]):
            bring(r, kv.at[d, core])
        bring(refs_of[7], kv.at[4, core, 0:256])
        bring(refs_of[8], kv.at[4, core, 256:512])
    for b in range(4):
        for t in range(4):
            g, m = t // 2, t % 2
            part = q_refs[b][g * 128 + m * 64 : g * 128 + m * 64 + 64, :]
            none = jnp.zeros((64, ROWS), BF16)
            queries[b * 4 + t, m * 64 : m * 64 + 64, :] = part
            queries[b * 4 + t, (1 - m) * 64 : (1 - m) * 64 + 64, :] = none
    maxima[...] = jnp.full(maxima.shape, NEG_BIG, F32)
    acc[...] = jnp.zeros(acc.shape, F32)
    for copy in copies:
        copy.wait()
    key_row = lax.broadcasted_iota(jnp.int32, (512, ROWS), 0)
    query_row = lax.broadcasted_iota(jnp.int32, (512, ROWS), 1) + c * ROWS
    attend(range(4), kv, 0, queries, maxima, acc, key_row <= query_row)
    for b, by in ((1, 1), (2, -1), (3, 2)):

        @pl.when(lax.rem(y - by + 4, 4) > y)
        def _(b=b):
            attend(range(4 * b, 4 * b + 4), kv, 0, queries, maxima, acc)

    def visit(d, carry):
        attend(range(16), kv, d, queries, maxima, acc)
        return carry

    lax.fori_loop(1, z + 1, visit, 0)
    for b in range(4):
        lines = []
        for t in range(4):
            i = b * 4 + t
            length = acc[i, VDIM : VDIM + 1, :]
            some = length > 0.0
            safe = jnp.where(some, length, 1.0)
            outs[b][t * VDIM : (t + 1) * VDIM, :] = (acc[i, 0:VDIM, :] / safe).astype(BF16)
            log = jnp.where(some, maxima[i] + jnp.log(safe), NEG_BIG)
            for _ in range(3):
                piece = log.astype(BF16).astype(F32)
                lines.append(piece)
                log = log - piece
        lines.append(jnp.zeros((4, ROWS), F32))
        outs[b][4 * VDIM : MSG, :] = jnp.concatenate(lines, axis=0).astype(BF16)


def output_kernel(m0, m1, m2, m3, y_conv, gates, lam, gain, out_conv, out_attn, o0, o1, o2, o3, rows):
    x = lax.axis_index("tp")
    logs = []
    for ref in (m0, m1, m2, m3):
        stats = ref[4 * VDIM : MSG, :].astype(F32)
        logs.append([(stats[3 * t : 3 * t + 1] + stats[3 * t + 1 : 3 * t + 2]) + stats[3 * t + 2 : 3 * t + 3] for t in range(4)])
    for j in range(4):
        rows[j, :, 0:128] = y_conv[64 * j : 64 * j + 64, :]
    for g in range(2):
        maps = []
        for m in range(2):
            t = 2 * g + m
            top = functools.reduce(jnp.maximum, [l[t] for l in logs])
            weights = [jnp.exp(l[t] - top) for l in logs]
            norm = 1.0 / functools.reduce(jnp.add, weights)
            part = [r[t * VDIM : (t + 1) * VDIM, :].astype(F32) * (w * norm) for r, w in zip((m0, m1, m2, m3), weights)]
            maps.append((part[0] + part[1]) + (part[2] + part[3]))
        o = maps[0] - lam[g] * maps[1]
        o = o * lax.rsqrt(jnp.mean(o * o, axis=0, keepdims=True) + EPSILON)
        o = jnp.transpose(o) * gain[...] * HEAD_SCALE
        gate = gates[:, 128 + g * 128 : 256 + g * 128].astype(F32)
        o = (o * jax.nn.silu(gate)).astype(BF16)
        for j in range(4):
            rows[j, :, 128 + g * 128 : 256 + g * 128] = o[64 * j : 64 * j + 64, :]
    order = [lax.rem(x + by + 4, 4) for by in (0,) + SHIFTS]
    ordered = jnp.concatenate([rows[j] for j in order], axis=0)
    total = dot(ordered[:, 0:128], out_conv[...]) + dot(ordered[:, 128:384], out_attn[...])
    for i, ref in enumerate((o0, o1, o2, o3)):
        ref[...] = total[64 * i : 64 * i + 64, :].astype(BF16)


def shape(dims, kind=BF16):
    return jax.ShapeDtypeStruct(dims, kind)


def local(
    tokens,
    in_gain,
    w_glu_value,
    w_glu_gate,
    w_query,
    w_key,
    w_value,
    w_gate_conv,
    w_gate_attn,
    conv_weight,
    conv_gain,
    lam,
    head_gain,
    out_conv,
    out_attn,
):
    pieces = [tokens] + [tp_shift(tokens, by) for by in SHIFTS]
    gain = in_gain.astype(F32).reshape(4, 512)
    qt, kv, glued, tail, gates = pl.pallas_call(
        project_kernel,
        out_shape=[shape((256, ROWS)), shape((512, 128)), shape((ROWS, 128)), shape((32, 128)), shape((ROWS, 384))],
        in_specs=[VM] * 12,
        out_specs=[VM] * 5,
        scratch_shapes=[pltpu.VMEM((4, ROWS, 512), BF16)],
        compiler_params=BIG,
        name="project",
    )(*pieces, gain, w_glu_value, w_glu_gate, w_query, w_key, w_value, w_gate_conv, w_gate_attn)

    p1, m1, p2, m2 = [z_shift(kv, by) for by in (1, -1, 2, -2)]
    q_blocks = [qt] + [y_shift(qt, by) for by in SHIFTS]
    s_next = [(i, i + 1) for i in range(63)]
    before = lax.ppermute(tail, "sp", s_next)
    p3, m3 = z_shift(p2, 1), z_shift(m2, -1)
    p4, m4 = z_shift(p2[0:256], 2), z_shift(m2[256:512], -2)
    kv_own = [kv, p1, m1, p2, m2, p3, m3, p4, m4]
    kv_other = [core_swap(k) for k in kv_own]

    conv, squares = pl.pallas_call(
        conv_kernel,
        out_shape=[shape((ROWS, 128), F32), shape((1, ROWS), F32)],
        in_specs=[VM] * 3,
        out_specs=[VM] * 2,
        scratch_shapes=[pltpu.VMEM((32 + ROWS, 128), F32)],
        name="conv",
    )(glued, before, conv_weight)
    sums = [squares] + [tp_shift(squares, by) for by in SHIFTS]
    y_conv = pl.pallas_call(
        gate_kernel,
        out_shape=shape((ROWS, 128)),
        in_specs=[VM] * 7,
        out_specs=VM,
        name="gate",
    )(conv, *sums, conv_gain.reshape(1, 128), gates)

    parts = pl.pallas_call(
        attention_kernel,
        out_shape=[shape((MSG, ROWS))] * 4,
        in_specs=[VM] * 4 + [ANY] * 18,
        out_specs=[VM] * 4,
        scratch_shapes=[
            pltpu.VMEM((8, 2, 512, 128), BF16),
            pltpu.VMEM((16, 128, ROWS), BF16),
            pltpu.VMEM((16, 1, ROWS), F32),
            pltpu.VMEM((16, ACC, ROWS), F32),
            pltpu.SemaphoreType.DMA((18,)),
        ],
        compiler_params=BIG,
        name="attention",
    )(*q_blocks, *kv_own, *kv_other)
    merged = [parts[0]] + [y_shift(part, -by) for part, by in zip(parts[1:], SHIFTS)]

    outs = pl.pallas_call(
        output_kernel,
        out_shape=[shape((64, D))] * 4,
        in_specs=[VM] * 6 + [SM] + [VM] * 3,
        out_specs=[VM] * 4,
        scratch_shapes=[pltpu.VMEM((4, 64, 384), BF16)],
        compiler_params=BIG,
        name="output",
    )(*merged, y_conv, gates, lam, head_gain.reshape(1, 128), out_conv, out_attn)
    sums = [outs[0]] + [tp_shift(o, by) for o, by in zip(outs[1:], SHIFTS)]
    a, b, c, d = [o.astype(F32) for o in sums]
    return ((a + b) + (c + d)).astype(BF16)


def solution(mesh):
    in_specs = (
        P("sp", "tp"),
        P(),
        P(None, "tp"),
        P(None, "tp"),
        P(None, "tp"),
        P(None, "tp"),
        P(None, "tp"),
        P(None, "tp"),
        P(None, "tp"),
        P(None, "tp"),
        P("tp"),
        P("tp"),
        P(),
        P("tp", None),
        P("tp", None),
    )
    out_specs = P(("sp", "tp"), None)
    return jax.shard_map(local, mesh=mesh, in_specs=in_specs, out_specs=out_specs, check_vma=False)
```

```python
import functools

import jax
import jax.numpy as jnp
from jax import lax
from jax.experimental import pallas as pl
from jax.experimental.pallas import tpu as pltpu
from jax.sharding import PartitionSpec as P


D = 2048
CONV = 512
QK = 64
VDIM = 128
WIDTH = 31
ROWS = 256
ACC = VDIM + 16
MSG = 4 * VDIM + 16

EPSILON = 1e-06
NEG_BIG = -1e30
HEAD_SCALE = 0.8


F32 = jnp.float32
BF16 = jnp.bfloat16
VM = pl.BlockSpec(memory_space=pltpu.VMEM)
OUT = pl.BlockSpec()
SM = pl.BlockSpec(memory_space=pltpu.SMEM)
ANY = pl.BlockSpec(memory_space=pltpu.MemorySpace.HBM)
BIG = pltpu.CompilerParams(vmem_limit_bytes=56 * 1024 * 1024)
SHIFTS = (1, -1, 2)
DEPTH = 3
LOG2E = 1.4426950408889634


def place(s):
    return s // 8, (s // 2) % 4, s % 2


def along_sp(x, move):
    pairs = []
    for s in range(64):
        z, y, c = place(s)
        z, y, c = move(z, y, c)
        pairs.append((s, z * 8 + y * 2 + c))
    return lax.ppermute(x, "sp", pairs)


def z_shift(x, by):
    return along_sp(x, lambda z, y, c: ((z + by) % 8, y, c))


def y_shift(x, by):
    return along_sp(x, lambda z, y, c: (z, (y + by) % 4, c))


def core_swap(x):
    return along_sp(x, lambda z, y, c: (z, y, 1 - c))


def tp_shift(x, by):
    return lax.ppermute(x, "tp", [(i, (i + by) % 4) for i in range(4)])


def dot(a, b):
    return jnp.dot(a, b, preferred_element_type=F32)


def fetch(pairs, sems):
    copies = [pltpu.make_async_copy(src, dst, sems.at[i]) for i, (src, dst) in enumerate(pairs)]
    for copy in copies:
        copy.start()
    return copies


def project_kernel(t0, t1, t2, t3, gain, wq, wk, wv, qt, kv, scaled, inv_out, tok, vq, vk, vv, sems):
    x = lax.axis_index("tp")
    copies = fetch([(t, tok.at[i]) for i, t in enumerate((t0, t1, t2, t3))] + [(wk, vk), (wv, vv), (wq, vq)], sems)
    squares = jnp.zeros((ROWS, 128), F32)
    for i, by in enumerate((0,) + SHIFTS):
        j = lax.rem(x - by + 4, 4)
        copies[i].wait()
        wide = tok[i].astype(F32)
        scaled[j] = (wide * gain[pl.ds(j, 1), :]).astype(BF16)
        sq = wide * wide
        squares += (sq[:, 0:128] + sq[:, 128:256]) + (sq[:, 256:384] + sq[:, 384:512])
    inv = lax.rsqrt(jnp.sum(squares, axis=1, keepdims=True) / D + EPSILON)
    inv_out[...] = jnp.broadcast_to(inv, (ROWS, 128))
    rows = jnp.concatenate([scaled[j] for j in range(4)], axis=1)
    copies[4].wait()
    copies[5].wait()
    both = dot(rows, jnp.concatenate([vk[...], vv[...]], axis=1)) * inv
    kv[0:256, :] = both[:, 0:128].astype(BF16)
    vt = jnp.transpose(both[:, 128:256]).astype(BF16)
    kv[256:384, :] = vt[:, 0:128]
    kv[384:512, :] = vt[:, 128:256]
    copies[6].wait()
    q = dot(rows, vq[...]) * inv
    qt[...] = jnp.transpose(q * (QK ** -0.5)).astype(BF16)


def rest_kernel(scaled, inv_in, wgv, wgg, wgc, wga, glued, tail, gates):
    inv = inv_in[...]
    wide = jnp.concatenate([inv, inv], axis=1)
    rows = jnp.concatenate([scaled[j] for j in range(4)], axis=1)
    glu = (dot(rows, jnp.concatenate([wgv[...], wgg[...]], axis=1)) * wide).astype(BF16).astype(F32)
    g = (glu[:, 0:128] * jax.nn.sigmoid(glu[:, 128:256])).astype(BF16)
    glued[...] = g
    tail[...] = g[ROWS - 32 :, :]
    gates[:, 0:128] = (dot(rows, wgc[...]) * inv).astype(BF16)
    gates[:, 128:384] = (dot(rows, wga[...]) * wide).astype(BF16)


def conv_kernel(glued, before, weight, conv, squares, padded):
    padded[0:32, :] = before[...].astype(F32)
    padded[32 : 32 + ROWS, :] = glued[...].astype(F32)
    taps = weight[...].astype(F32)
    total = jnp.zeros((ROWS, 128), F32)
    for j in range(WIDTH):
        total += padded[j + 2 : j + 2 + ROWS, :] * taps[j : j + 1, :]
    conv[...] = total
    squares[...] = jnp.sum(jnp.transpose(total * total), axis=0, keepdims=True)


def gate_kernel(conv, s0, s1, s2, s3, gain, gates, y_conv):
    total = (s0[...] + s1[...]) + (s2[...] + s3[...])
    inv = lax.rsqrt(total / CONV + EPSILON)
    inv = jnp.transpose(jnp.broadcast_to(inv, (128, ROWS)))
    normed = conv[...] * inv * gain[...]
    y_conv[...] = (jax.nn.silu(normed) * jax.nn.silu(gates[:, 0:128].astype(F32))).astype(BF16)


def attend(tiles, kv, slot, queries, maxima, acc, mask=None):
    keys = jnp.concatenate([kv[slot, 0, 0:256, :], kv[slot, 1, 0:256, :]], axis=0)
    keys = jnp.concatenate([keys, keys], axis=1)
    values = jnp.concatenate(
        [
            kv[slot, 0, 256:384, :],
            kv[slot, 0, 384:512, :],
            kv[slot, 1, 256:384, :],
            kv[slot, 1, 384:512, :],
        ],
        axis=1,
    )
    values = jnp.concatenate([values, jnp.ones((ACC - VDIM, 512), BF16)], axis=0)
    ahead = [dot(keys, queries[t]) for t in tiles[:DEPTH]]
    for i, t in enumerate(tiles):
        scores = ahead.pop(0)
        if i + DEPTH < len(tiles):
            ahead.append(dot(keys, queries[tiles[i + DEPTH]]))
        if mask is not None:
            scores = jnp.where(mask, scores, NEG_BIG)
        old = maxima[t]
        new = jnp.maximum(old, jnp.max(scores, axis=0, keepdims=True))
        factor = jnp.exp2(old - new)
        expd = jnp.exp2(scores - new).astype(BF16)
        acc[t] = acc[t] * factor + dot(values, expd)
        maxima[t] = new


def lay_queries(q_refs, queries):
    none = jnp.zeros((64, ROWS), BF16)
    for b, ref in enumerate(q_refs):
        for t in range(4):
            g, m = t // 2, t % 2
            part = ref[g * 128 + m * 64 : g * 128 + m * 64 + 64, :].astype(F32) * LOG2E
            high = part.astype(BF16)
            low = (part - high.astype(F32)).astype(BF16)
            for i, rows in enumerate((high, low)):
                at = i * 128
                queries[b * 4 + t, at + m * 64 : at + m * 64 + 64, :] = rows
                queries[b * 4 + t, at + (1 - m) * 64 : at + (1 - m) * 64 + 64, :] = none


def write_part(out, first, maxima, acc):
    lines = []
    for t in range(4):
        i = first + t
        length = acc[i, VDIM : VDIM + 1, :]
        some = length > 0.0
        safe = jnp.where(some, length, 1.0)
        out[t * VDIM : (t + 1) * VDIM, :] = (acc[i, 0:VDIM, :] * (1.0 / safe)).astype(BF16)
        log = jnp.where(some, maxima[i] + jnp.log2(safe), NEG_BIG)
        for _ in range(3):
            piece = log.astype(BF16).astype(F32)
            lines.append(piece)
            log = log - piece
    lines.append(jnp.zeros((4, ROWS), F32))
    out[4 * VDIM : MSG, :] = jnp.concatenate(lines, axis=0).astype(BF16)


def position():
    s = lax.axis_index("sp")
    return s // 8, lax.rem(s // 2, 4), lax.rem(s, 2)


def kv_pairs(refs, kv, slots, core):
    pairs = []
    for ref, slot in zip(refs, slots):
        if isinstance(ref, tuple):
            pairs += [(ref[0], kv.at[slot, core, 0:256]), (ref[1], kv.at[slot, core, 256:512])]
        else:
            pairs.append((ref, kv.at[slot, core]))
    return pairs


def loop_over(tiles, kv, count, first, queries, maxima, acc):
    def visit(i, carry):
        attend(tiles, kv, first + i, queries, maxima, acc)
        return carry

    lax.fori_loop(0, count, visit, 0)


def early_kernel(*refs):
    q_refs, own, other = refs[0:3], refs[3:8], refs[8:13]
    max_out, acc_out, kv, queries, maxima, sems = refs[13:]
    acc = acc_out
    z, y, c = position()
    slots = (0, 1, 4, 2, 3)
    copies = fetch(kv_pairs(own, kv, slots, c) + kv_pairs(other, kv, slots, 1 - c), sems)
    lay_queries(q_refs, queries)
    maxima[...] = jnp.full(maxima.shape, NEG_BIG, F32)
    acc[...] = jnp.zeros(acc.shape, F32)
    for copy in copies:
        copy.wait()
    for b, by in enumerate(SHIFTS):

        @pl.when(lax.rem(y - by + 4, 4) > y)
        def _(b=b):
            attend(range(4 * b, 4 * b + 4), kv, 0, queries, maxima, acc)

    count = jnp.minimum(z, 2) + jnp.where(z >= 6, 1, 0) + jnp.where(z >= 7, 1, 0)
    loop_over(range(12), kv, count, 1, queries, maxima, acc)
    max_out[...] = maxima[...]


def late_kernel(*refs, blocks):
    n = len(blocks)
    q_refs, own, other = refs[0:n], refs[n : n + 4], refs[n + 4 : n + 8]
    max_in, acc_in = refs[n + 8 : n + 10]
    outs = refs[n + 10 : 2 * n + 10]
    kv, queries, maxima, acc, sems = refs[2 * n + 10 :]
    z, _, c = position()
    pairs = [((own[2], own[3])), ((other[2], other[3]))]
    slots = (0, 2, 1)
    copies = fetch(
        kv_pairs((own[0], own[1], pairs[0]), kv, slots, c)
        + kv_pairs((other[0], other[1], pairs[1]), kv, slots, 1 - c)
        + [(max_in.at[4 * b : 4 * b + 4], maxima.at[4 * i : 4 * i + 4]) for i, b in enumerate(blocks)]
        + [(acc_in.at[4 * b : 4 * b + 4], acc.at[4 * i : 4 * i + 4]) for i, b in enumerate(blocks)],
        sems,
    )
    lay_queries(q_refs, queries)
    for copy in copies:
        copy.wait()
    loop_over(range(4 * n), kv, jnp.clip(z - 2, 0, 3), 0, queries, maxima, acc)
    for i in range(n):
        write_part(outs[i], 4 * i, maxima, acc)


def self_kernel(*refs):
    q_ref, own, other, out = refs[0], refs[1:10], refs[10:19], refs[19]
    kv, queries, maxima, acc, sems = refs[20:]
    z, _, c = position()
    slots = (0, 1, 7, 2, 6, 3, 5, 4)
    copies = fetch(
        kv_pairs(own[0:7] + ((own[7], own[8]),), kv, slots, c)
        + kv_pairs(other[0:7] + ((other[7], other[8]),), kv, slots, 1 - c),
        sems,
    )
    lay_queries((q_ref,), queries)
    maxima[...] = jnp.full(maxima.shape, NEG_BIG, F32)
    acc[...] = jnp.zeros(acc.shape, F32)
    for copy in copies:
        copy.wait()
    key_row = lax.broadcasted_iota(jnp.int32, (512, ROWS), 0)
    query_row = lax.broadcasted_iota(jnp.int32, (512, ROWS), 1) + c * ROWS
    attend(range(4), kv, 0, queries, maxima, acc, key_row <= query_row)
    loop_over(range(4), kv, z, 1, queries, maxima, acc)
    write_part(out, 0, maxima, acc)


def output_kernel(m0, m1, m2, m3, y_conv, gates, lam, gain, out_conv, out_attn, o0, o1, o2, o3, rows):
    x = lax.axis_index("tp")
    logs = []
    for ref in (m0, m1, m2, m3):
        stats = ref[4 * VDIM : MSG, :].astype(F32)
        logs.append([(stats[3 * t : 3 * t + 1] + stats[3 * t + 1 : 3 * t + 2]) + stats[3 * t + 2 : 3 * t + 3] for t in range(4)])
    for j in range(4):
        rows[j, :, 0:128] = y_conv[64 * j : 64 * j + 64, :]
    for g in range(2):
        maps = []
        for m in range(2):
            t = 2 * g + m
            top = functools.reduce(jnp.maximum, [l[t] for l in logs])
            weights = [jnp.exp2(l[t] - top) for l in logs]
            norm = 1.0 / functools.reduce(jnp.add, weights)
            part = [r[t * VDIM : (t + 1) * VDIM, :].astype(F32) * (w * norm) for r, w in zip((m0, m1, m2, m3), weights)]
            maps.append((part[0] + part[1]) + (part[2] + part[3]))
        o = maps[0] - lam[g] * maps[1]
        o = o * lax.rsqrt(jnp.mean(o * o, axis=0, keepdims=True) + EPSILON)
        o = jnp.transpose(o) * gain[...] * HEAD_SCALE
        gate = gates[:, 128 + g * 128 : 256 + g * 128].astype(F32)
        o = (o * jax.nn.silu(gate)).astype(BF16)
        for j in range(4):
            rows[j, :, 128 + g * 128 : 256 + g * 128] = o[64 * j : 64 * j + 64, :]
    order = [lax.rem(x + by + 4, 4) for by in (0,) + SHIFTS]
    ordered = jnp.concatenate([rows[j] for j in order], axis=0)
    total = dot(ordered[:, 0:128], out_conv[...]) + dot(ordered[:, 128:384], out_attn[...])
    for i, ref in enumerate((o0, o1, o2, o3)):
        ref[...] = total[64 * i : 64 * i + 64, :].astype(BF16)


def in_hbm(arrays):
    return [pltpu.with_memory_space_constraint(a, pltpu.MemorySpace.HBM) for a in arrays]


def shape(dims, kind=BF16):
    return jax.ShapeDtypeStruct(dims, kind)


def sent(dims, kind=BF16):
    return pltpu.MemorySpace.HBM(dims, kind)


def local(
    tokens,
    in_gain,
    w_glu_value,
    w_glu_gate,
    w_query,
    w_key,
    w_value,
    w_gate_conv,
    w_gate_attn,
    conv_weight,
    conv_gain,
    lam,
    head_gain,
    out_conv,
    out_attn,
):
    pieces = [tokens] + [tp_shift(tokens, by) for by in SHIFTS]
    gain = in_gain.astype(F32).reshape(4, 512)
    qt, kv, scaled, inv = pl.pallas_call(
        project_kernel,
        out_shape=[sent((256, ROWS)), sent((512, 128)), shape((4, ROWS, 512)), shape((ROWS, 128), F32)],
        in_specs=[ANY] * 4 + [VM] + [ANY] * 3,
        out_specs=[OUT] * 2 + [VM] * 2,
        scratch_shapes=[
            pltpu.VMEM((4, ROWS, 512), BF16),
            pltpu.VMEM((D, 256), BF16),
            pltpu.VMEM((D, 128), BF16),
            pltpu.VMEM((D, 128), BF16),
            pltpu.SemaphoreType.DMA((7,)),
        ],
        compiler_params=BIG,
        name="project",
    )(*in_hbm(pieces), gain, *in_hbm([w_query, w_key, w_value]))

    p2, m2, p1, m1 = [z_shift(kv, by) for by in (2, -2, 1, -1)]
    kv_s = core_swap(kv)
    q_blocks = [y_shift(qt, by) for by in SHIFTS]

    glued, tail, gates = pl.pallas_call(
        rest_kernel,
        out_shape=[shape((ROWS, 128)), sent((32, 128)), shape((ROWS, 384))],
        in_specs=[VM] * 6,
        out_specs=[VM, OUT, VM],
        compiler_params=BIG,
        name="rest",
    )(scaled, inv, w_glu_value, w_glu_gate, w_gate_conv, w_gate_attn)
    before = lax.ppermute(tail, "sp", [(i, i + 1) for i in range(63)])
    conv, squares = pl.pallas_call(
        conv_kernel,
        out_shape=[shape((ROWS, 128), F32), sent((1, ROWS), F32)],
        in_specs=[VM] * 3,
        out_specs=[VM, OUT],
        scratch_shapes=[pltpu.VMEM((32 + ROWS, 128), F32)],
        name="conv",
    )(glued, before, conv_weight)
    sums = [squares] + [tp_shift(squares, by) for by in SHIFTS]

    (p1, m1, p2, m2), squares = lax.optimization_barrier(((p1, m1, p2, m2), squares))
    p3, m3 = z_shift(p2, 1), z_shift(m2, -1)
    p4, m4 = z_shift(p2[0:256], 2), z_shift(m2[256:512], -2)
    near = [kv, p1, m1, p2, m2]
    near_s = [kv_s] + [core_swap(k) for k in near[1:]]

    y_conv = pl.pallas_call(
        gate_kernel,
        out_shape=shape((ROWS, 128)),
        in_specs=[VM] * 7,
        out_specs=VM,
        name="gate",
    )(conv, *sums, conv_gain.reshape(1, 128), gates)
    y_conv, near_s = lax.optimization_barrier((y_conv, near_s))

    def scratch(slots, tiles, held, copies):
        return (
            [pltpu.VMEM((slots, 2, 512, 128), BF16), pltpu.VMEM((tiles, 256, ROWS), BF16), pltpu.VMEM((tiles, 1, ROWS), F32)]
            + ([pltpu.VMEM((tiles, ACC, ROWS), F32)] if held else [])
            + [pltpu.SemaphoreType.DMA((copies,))]
        )

    maxima, acc = pl.pallas_call(
        early_kernel,
        out_shape=[shape((12, 1, ROWS), F32), shape((12, ACC, ROWS), F32)],
        in_specs=[VM] * 3 + [ANY] * 10,
        out_specs=[VM] * 2,
        scratch_shapes=scratch(5, 12, False, 10),
        compiler_params=BIG,
        name="early",
    )(*q_blocks, *in_hbm(near), *in_hbm(near_s))

    (p3, m3, p4, m4), acc = lax.optimization_barrier(((p3, m3, p4, m4), acc))
    far = [p3, m3, p4, m4]
    far_s = [core_swap(k) for k in far]

    def late(blocks, acc):
        n = len(blocks)
        return pl.pallas_call(
            functools.partial(late_kernel, blocks=blocks),
            out_shape=[sent((MSG, ROWS))] * n,
            in_specs=[VM] * n + [ANY] * 8 + [pl.BlockSpec(memory_space=pl.ANY)] * 2,
            out_specs=[OUT] * n,
            scratch_shapes=scratch(3, 4 * n, True, 8 + 2 * n),
            compiler_params=BIG,
        )(*[q_blocks[b] for b in blocks], *in_hbm(far), *in_hbm(far_s), maxima, acc)

    (part2,) = late((2,), acc)
    part2, acc = lax.optimization_barrier((part2, acc))
    back2 = y_shift(part2, -2)
    part0, part1 = late((0, 1), acc)
    back0, back1 = y_shift(part0, -1), y_shift(part1, 1)
    (part0, qt) = lax.optimization_barrier((part0, qt))
    part = pl.pallas_call(
        self_kernel,
        out_shape=shape((MSG, ROWS)),
        in_specs=[VM] + [ANY] * 18,
        out_specs=VM,
        scratch_shapes=scratch(8, 4, True, 18),
        compiler_params=BIG,
        name="self",
    )(qt, *in_hbm(near), *in_hbm(far), *in_hbm(near_s), *in_hbm(far_s))
    merged = [part, back0, back1, back2]

    outs = pl.pallas_call(
        output_kernel,
        out_shape=[sent((64, D))] * 4,
        in_specs=[VM] * 6 + [SM] + [VM] * 3,
        out_specs=[OUT] * 4,
        scratch_shapes=[pltpu.VMEM((4, 64, 384), BF16)],
        compiler_params=BIG,
        name="output",
    )(*merged, y_conv, gates, lam, head_gain.reshape(1, 128), out_conv, out_attn)
    sums = [outs[0]] + [tp_shift(o, by) for o, by in zip(outs[1:], SHIFTS)]
    a, b, c, d = [o.astype(F32) for o in sums]
    return ((a + b) + (c + d)).astype(BF16)


def solution(mesh):
    in_specs = (
        P("sp", "tp"),
        P(),
        P(None, "tp"),
        P(None, "tp"),
        P(None, "tp"),
        P(None, "tp"),
        P(None, "tp"),
        P(None, "tp"),
        P(None, "tp"),
        P(None, "tp"),
        P("tp"),
        P("tp"),
        P(),
        P("tp", None),
        P("tp", None),
    )
    out_specs = P(("sp", "tp"), None)

    return jax.shard_map(local, mesh=mesh, in_specs=in_specs, out_specs=out_specs, check_vma=False)
```

```python
import functools

import jax
import jax.numpy as jnp
from jax import lax
from jax.experimental import pallas as pl
from jax.experimental.pallas import tpu as pltpu
from jax.sharding import PartitionSpec as P


D = 2048
CONV = 512
QK = 64
VDIM = 128
WIDTH = 31
ROWS = 256
ACC = VDIM + 16
MSG = 4 * VDIM + 16

EPSILON = 1e-06
NEG_BIG = -1e30
HEAD_SCALE = 0.8


F32 = jnp.float32
BF16 = jnp.bfloat16
VM = pl.BlockSpec(memory_space=pltpu.VMEM)
OUT = pl.BlockSpec()
SM = pl.BlockSpec(memory_space=pltpu.SMEM)
ANY = pl.BlockSpec(memory_space=pltpu.MemorySpace.HBM)
BIG = pltpu.CompilerParams(vmem_limit_bytes=56 * 1024 * 1024)
SHIFTS = (1, -1, 2)
DEPTH = 3
LOG2E = 1.4426950408889634


def place(s):
    return s // 8, (s // 2) % 4, s % 2


def along_sp(x, move):
    pairs = []
    for s in range(64):
        z, y, c = place(s)
        z, y, c = move(z, y, c)
        pairs.append((s, z * 8 + y * 2 + c))
    return lax.ppermute(x, "sp", pairs)


def y_shift(x, by):
    return along_sp(x, lambda z, y, c: (z, (y + by) % 4, c))


def core_swap(x):
    return along_sp(x, lambda z, y, c: (z, y, 1 - c))


def tp_shift(x, by):
    return lax.ppermute(x, "tp", [(i, (i + by) % 4) for i in range(4)])


def dot(a, b):
    return jnp.dot(a, b, preferred_element_type=F32)


def fetch(pairs, sems):
    copies = [pltpu.make_async_copy(src, dst, sems.at[i]) for i, (src, dst) in enumerate(pairs)]
    for copy in copies:
        copy.start()
    return copies


def project_kernel(t0, t1, t2, t3, gain, wq, wk, wv, qt, kv, scaled, inv_out, tok, vq, vk, vv, sems):
    x = lax.axis_index("tp")
    copies = fetch([(t, tok.at[i]) for i, t in enumerate((t0, t1, t2, t3))] + [(wk, vk), (wv, vv), (wq, vq)], sems)
    squares = jnp.zeros((ROWS, 128), F32)
    for i, by in enumerate((0,) + SHIFTS):
        j = lax.rem(x - by + 4, 4)
        copies[i].wait()
        wide = tok[i].astype(F32)
        scaled[j] = (wide * gain[pl.ds(j, 1), :]).astype(BF16)
        sq = wide * wide
        squares += (sq[:, 0:128] + sq[:, 128:256]) + (sq[:, 256:384] + sq[:, 384:512])
    inv = lax.rsqrt(jnp.sum(squares, axis=1, keepdims=True) / D + EPSILON)
    inv_out[...] = jnp.broadcast_to(inv, (ROWS, 128))
    rows = jnp.concatenate([scaled[j] for j in range(4)], axis=1)
    copies[4].wait()
    copies[5].wait()
    both = dot(rows, jnp.concatenate([vk[...], vv[...]], axis=1)) * inv
    k = both[:, 0:128].astype(BF16)
    vt = jnp.transpose(both[:, 128:256]).astype(BF16)
    for z in range(8):
        kv[z, 0:256, :] = k
        kv[z, 256:384, :] = vt[:, 0:128]
        kv[z, 384:512, :] = vt[:, 128:256]
    copies[6].wait()
    q = dot(rows, vq[...]) * inv
    qt[...] = jnp.transpose(q * (QK ** -0.5)).astype(BF16)


def rest_kernel(scaled, inv_in, wgv, wgg, wgc, wga, glued, tail, gates):
    inv = inv_in[...]
    wide = jnp.concatenate([inv, inv], axis=1)
    rows = jnp.concatenate([scaled[j] for j in range(4)], axis=1)
    glu = (dot(rows, jnp.concatenate([wgv[...], wgg[...]], axis=1)) * wide).astype(BF16).astype(F32)
    g = (glu[:, 0:128] * jax.nn.sigmoid(glu[:, 128:256])).astype(BF16)
    glued[...] = g
    tail[...] = g[ROWS - 32 :, :]
    gates[:, 0:128] = (dot(rows, wgc[...]) * inv).astype(BF16)
    gates[:, 128:384] = (dot(rows, wga[...]) * wide).astype(BF16)


def conv_kernel(glued, before, weight, conv, squares, padded):
    padded[0:32, :] = before[...].astype(F32)
    padded[32 : 32 + ROWS, :] = glued[...].astype(F32)
    taps = weight[...].astype(F32)
    total = jnp.zeros((ROWS, 128), F32)
    for j in range(WIDTH):
        total += padded[j + 2 : j + 2 + ROWS, :] * taps[j : j + 1, :]
    conv[...] = total
    squares[...] = jnp.sum(jnp.transpose(total * total), axis=0, keepdims=True)


def attend(tiles, kv, slot, queries, maxima, acc, mask=None):
    keys = jnp.concatenate([kv[0, slot, 0:256, :], kv[1, slot, 0:256, :]], axis=0)
    keys = jnp.concatenate([keys, keys], axis=1)
    values = jnp.concatenate(
        [
            kv[0, slot, 256:384, :],
            kv[0, slot, 384:512, :],
            kv[1, slot, 256:384, :],
            kv[1, slot, 384:512, :],
        ],
        axis=1,
    )
    values = jnp.concatenate([values, jnp.ones((ACC - VDIM, 512), BF16)], axis=0)
    ahead = [dot(keys, queries[t]) for t in tiles[:DEPTH]]
    for i, t in enumerate(tiles):
        scores = ahead.pop(0)
        if i + DEPTH < len(tiles):
            ahead.append(dot(keys, queries[tiles[i + DEPTH]]))
        if mask is not None:
            scores = jnp.where(mask, scores, NEG_BIG)
        old = maxima[t]
        new = jnp.maximum(old, jnp.max(scores, axis=0, keepdims=True))
        factor = jnp.exp2(old - new)
        expd = jnp.exp2(scores - new).astype(BF16)
        acc[t] = acc[t] * factor + dot(values, expd)
        maxima[t] = new


def lay_queries(q_refs, queries):
    none = jnp.zeros((64, ROWS), BF16)
    for b, ref in enumerate(q_refs):
        for t in range(4):
            g, m = t // 2, t % 2
            part = ref[g * 128 + m * 64 : g * 128 + m * 64 + 64, :].astype(F32) * LOG2E
            high = part.astype(BF16)
            low = (part - high.astype(F32)).astype(BF16)
            for i, rows in enumerate((high, low)):
                at = i * 128
                queries[b * 4 + t, at + m * 64 : at + m * 64 + 64, :] = rows
                queries[b * 4 + t, at + (1 - m) * 64 : at + (1 - m) * 64 + 64, :] = none


def write_part(out, first, maxima, acc):
    lines = []
    for t in range(4):
        i = first + t
        length = acc[i, VDIM : VDIM + 1, :]
        some = length > 0.0
        safe = jnp.where(some, length, 1.0)
        out[t * VDIM : (t + 1) * VDIM, :] = (acc[i, 0:VDIM, :] * (1.0 / safe)).astype(BF16)
        log = jnp.where(some, maxima[i] + jnp.log2(safe), NEG_BIG)
        for _ in range(3):
            piece = log.astype(BF16).astype(F32)
            lines.append(piece)
            log = log - piece
    lines.append(jnp.zeros((4, ROWS), F32))
    out[4 * VDIM : MSG, :] = jnp.concatenate(lines, axis=0).astype(BF16)


def position():
    s = lax.axis_index("sp")
    return s // 8, lax.rem(s // 2, 4), lax.rem(s, 2)


def bring(own, other, kv, sems):
    c = lax.rem(lax.axis_index("sp"), 2)
    return fetch([(own, kv.at[c]), (other, kv.at[1 - c])], sems)


def start_state(maxima, acc):
    maxima[...] = jnp.full(maxima.shape, NEG_BIG, F32)
    acc[...] = jnp.zeros(acc.shape, F32)


def remote_kernel(q0, q1, q2, own, other, o0, o1, o2, kv, queries, maxima, acc, sems):
    copies = bring(own, other, kv, sems)
    z, y, _ = position()
    lay_queries((q0, q1, q2), queries)
    start_state(maxima, acc)
    for copy in copies:
        copy.wait()

    def visit(i, carry):
        attend(range(12), kv, i, queries, maxima, acc)
        return carry

    lax.fori_loop(0, z, visit, 0)
    for b, by in enumerate(SHIFTS):

        @pl.when(lax.rem(y - by + 4, 4) > y)
        def _(b=b):
            attend(range(4 * b, 4 * b + 4), kv, z, queries, maxima, acc)

    for b, out in enumerate((o0, o1, o2)):
        write_part(out, 4 * b, maxima, acc)


def self_kernel(q0, own, other, out, kv, queries, maxima, acc, sems):
    copies = bring(own, other, kv, sems)
    z, _, c = position()
    lay_queries((q0,), queries)
    start_state(maxima, acc)
    for copy in copies:
        copy.wait()
    key_row = lax.broadcasted_iota(jnp.int32, (512, ROWS), 0)
    query_row = lax.broadcasted_iota(jnp.int32, (512, ROWS), 1) + c * ROWS
    attend(range(4), kv, z, queries, maxima, acc, key_row <= query_row)

    def visit(i, carry):
        attend(range(4), kv, i, queries, maxima, acc)
        return carry

    lax.fori_loop(0, z, visit, 0)
    write_part(out, 0, maxima, acc)


def merge_kernel(m0, m1, m2, m3, conv, s0, s1, s2, s3, c_gain, gates, lam, gain, y0, y1, y2, y3, rows):
    x = lax.axis_index("tp")
    total = (s0[...] + s1[...]) + (s2[...] + s3[...])
    inv = lax.rsqrt(total / CONV + EPSILON)
    inv = jnp.transpose(jnp.broadcast_to(inv, (128, ROWS)))
    normed = conv[...] * inv * c_gain[...]
    y_conv = (jax.nn.silu(normed) * jax.nn.silu(gates[:, 0:128].astype(F32))).astype(BF16)
    for j in range(4):
        rows[j, :, 0:128] = y_conv[64 * j : 64 * j + 64, :]
    logs = []
    for ref in (m0, m1, m2, m3):
        stats = ref[4 * VDIM : MSG, :].astype(F32)
        logs.append([(stats[3 * t : 3 * t + 1] + stats[3 * t + 1 : 3 * t + 2]) + stats[3 * t + 2 : 3 * t + 3] for t in range(4)])
    for g in range(2):
        maps = []
        for m in range(2):
            t = 2 * g + m
            top = functools.reduce(jnp.maximum, [l[t] for l in logs])
            weights = [jnp.exp2(l[t] - top) for l in logs]
            norm = 1.0 / functools.reduce(jnp.add, weights)
            part = [r[t * VDIM : (t + 1) * VDIM, :].astype(F32) * (w * norm) for r, w in zip((m0, m1, m2, m3), weights)]
            maps.append((part[0] + part[1]) + (part[2] + part[3]))
        o = maps[0] - lam[g] * maps[1]
        o = o * lax.rsqrt(jnp.mean(o * o, axis=0, keepdims=True) + EPSILON)
        o = jnp.transpose(o) * gain[...] * HEAD_SCALE
        gate = gates[:, 128 + g * 128 : 256 + g * 128].astype(F32)
        o = (o * jax.nn.silu(gate)).astype(BF16)
        for j in range(4):
            rows[j, :, 128 + g * 128 : 256 + g * 128] = o[64 * j : 64 * j + 64, :]
    for ref, by in zip((y0, y1, y2, y3), (0,) + SHIFTS):
        ref[...] = rows[lax.rem(x + by + 4, 4)]


def output_kernel(y0, y1, y2, y3, w_conv, w_attn, a1, a2, a3, b1, b2, b3, out, held, sems):
    c = lax.rem(lax.axis_index("sp"), 2)
    copies = fetch([(a, held.at[c, i]) for i, a in enumerate((a1, a2, a3))] + [(b, held.at[1 - c, i]) for i, b in enumerate((b1, b2, b3))], sems)
    y = y0[...]
    mine = [dot(y[:, 0:128], w_conv[:, h]) + dot(y[:, 128:384], w_attn[:, h]) for h in (slice(0, 1024), slice(1024, 2048))]
    for copy in copies:
        copy.wait()
    theirs = jnp.concatenate([y1[...], y2[...], y3[...]], axis=1)
    for h in range(2):
        weights = jnp.concatenate([held[h, i] for i in range(3)], axis=0)
        out[:, h * 1024 : (h + 1) * 1024] = (mine[h] + dot(theirs, weights)).astype(BF16)


def shape(dims, kind=BF16):
    return jax.ShapeDtypeStruct(dims, kind)


def sent(dims, kind=BF16):
    return pltpu.MemorySpace.HBM(dims, kind)


def local(
    tokens,
    in_gain,
    w_glu_value,
    w_glu_gate,
    w_query,
    w_key,
    w_value,
    w_gate_conv,
    w_gate_attn,
    conv_weight,
    conv_gain,
    lam,
    head_gain,
    out_conv,
    out_attn,
):
    c = lax.rem(lax.axis_index("sp"), 2)
    half = lax.dynamic_slice_in_dim(jnp.concatenate([out_conv, out_attn], axis=0), c * 1024, 1024, 1)
    pieces = [tokens] + [tp_shift(tokens, by) for by in SHIFTS]
    gain = in_gain.astype(F32).reshape(4, 512)
    qt, kv, scaled, inv = pl.pallas_call(
        project_kernel,
        out_shape=[sent((256, ROWS)), sent((8, 512, 128)), shape((4, ROWS, 512)), shape((ROWS, 128), F32)],
        in_specs=[ANY] * 4 + [VM] + [ANY] * 3,
        out_specs=[OUT] * 2 + [VM] * 2,
        scratch_shapes=[
            pltpu.VMEM((4, ROWS, 512), BF16),
            pltpu.VMEM((D, 256), BF16),
            pltpu.VMEM((D, 128), BF16),
            pltpu.VMEM((D, 128), BF16),
            pltpu.SemaphoreType.DMA((7,)),
        ],
        compiler_params=BIG,
        name="project",
    )(*pieces, gain, w_query, w_key, w_value)

    groups = [[z * 8 + r for z in range(8)] for r in range(8)]
    gathered = lax.all_to_all(kv, "sp", 0, 0, tiled=True, axis_index_groups=groups)
    q_blocks = [y_shift(qt, by) for by in SHIFTS]
    half, scaled = lax.optimization_barrier((half, scaled))
    weights = [tp_shift(half, by) for by in SHIFTS]

    glued, tail, gates = pl.pallas_call(
        rest_kernel,
        out_shape=[shape((ROWS, 128)), sent((32, 128)), shape((ROWS, 384))],
        in_specs=[VM] * 6,
        out_specs=[VM, OUT, VM],
        compiler_params=BIG,
        name="rest",
    )(scaled, inv, w_glu_value, w_glu_gate, w_gate_conv, w_gate_attn)
    before = lax.ppermute(tail, "sp", [(i, i + 1) for i in range(63)])
    conv, squares = pl.pallas_call(
        conv_kernel,
        out_shape=[shape((ROWS, 128), F32), sent((1, ROWS), F32)],
        in_specs=[VM] * 3,
        out_specs=[VM, OUT],
        scratch_shapes=[pltpu.VMEM((32 + ROWS, 128), F32)],
        name="conv",
    )(glued, before, conv_weight)
    sums = [squares] + [tp_shift(squares, by) for by in SHIFTS]

    swapped = core_swap(gathered)

    def scratch(tiles):
        return [
            pltpu.VMEM((2, 8, 512, 128), BF16),
            pltpu.VMEM((tiles, 256, ROWS), BF16),
            pltpu.VMEM((tiles, 1, ROWS), F32),
            pltpu.VMEM((tiles, ACC, ROWS), F32),
            pltpu.SemaphoreType.DMA((2,)),
        ]

    parts = pl.pallas_call(
        remote_kernel,
        out_shape=[sent((MSG, ROWS))] * 3,
        in_specs=[VM] * 3 + [ANY] * 2,
        out_specs=[OUT] * 3,
        scratch_shapes=scratch(12),
        compiler_params=BIG,
        name="remote",
    )(*q_blocks, gathered, swapped)
    back = [y_shift(part, -by) for part, by in zip(parts, SHIFTS)]
    parts, qt, weights = lax.optimization_barrier((parts, qt, weights))
    weights_s = [core_swap(w) for w in weights]
    part = pl.pallas_call(
        self_kernel,
        out_shape=shape((MSG, ROWS)),
        in_specs=[VM] + [ANY] * 2,
        out_specs=VM,
        scratch_shapes=scratch(4),
        compiler_params=BIG,
        name="self",
    )(qt, gathered, swapped)

    rows = pl.pallas_call(
        merge_kernel,
        out_shape=[shape((64, 384))] + [sent((64, 384))] * 3,
        in_specs=[VM] * 11 + [SM, VM],
        out_specs=[VM] + [OUT] * 3,
        scratch_shapes=[pltpu.VMEM((4, 64, 384), BF16)],
        compiler_params=BIG,
        name="merge",
    )(part, *back, conv, *sums, conv_gain.reshape(1, 128), gates, lam, head_gain.reshape(1, 128))
    rows = [rows[0]] + [tp_shift(r, by) for r, by in zip(rows[1:], SHIFTS)]
    return pl.pallas_call(
        output_kernel,
        out_shape=shape((64, D)),
        in_specs=[VM] * 6 + [ANY] * 6,
        out_specs=VM,
        scratch_shapes=[pltpu.VMEM((2, 3, 384, 1024), BF16), pltpu.SemaphoreType.DMA((6,))],
        compiler_params=BIG,
        name="output",
    )(*rows, out_conv, out_attn, *weights, *weights_s)


def solution(mesh):
    in_specs = (
        P("sp", "tp"),
        P(),
        P(None, "tp"),
        P(None, "tp"),
        P(None, "tp"),
        P(None, "tp"),
        P(None, "tp"),
        P(None, "tp"),
        P(None, "tp"),
        P(None, "tp"),
        P("tp"),
        P("tp"),
        P(),
        P("tp", None),
        P("tp", None),
    )
    out_specs = P(("sp", "tp"), None)

    return jax.shard_map(local, mesh=mesh, in_specs=in_specs, out_specs=out_specs, check_vma=False)
```

```python
import functools

import jax
import jax.numpy as jnp
from jax import lax
from jax.experimental import pallas as pl
from jax.experimental.pallas import tpu as pltpu
from jax.sharding import PartitionSpec as P


D = 2048
CONV = 512
QK = 64
VDIM = 128
WIDTH = 31
ROWS = 256
ACC = VDIM + 16
MSG = 4 * VDIM + 16

EPSILON = 1e-06
NEG_BIG = -1e30
HEAD_SCALE = 0.8


F32 = jnp.float32
BF16 = jnp.bfloat16
VM = pl.BlockSpec(memory_space=pltpu.VMEM)
OUT = pl.BlockSpec()
SM = pl.BlockSpec(memory_space=pltpu.SMEM)
ANY = pl.BlockSpec(memory_space=pltpu.MemorySpace.HBM)
BIG = pltpu.CompilerParams(vmem_limit_bytes=56 * 1024 * 1024)
SHIFTS = (1, -1, 2)
DEPTH = 3
LOG2E = 1.4426950408889634


def place(s):
    return s // 8, (s // 2) % 4, s % 2


def along_sp(x, move):
    pairs = []
    for s in range(64):
        z, y, c = place(s)
        z, y, c = move(z, y, c)
        pairs.append((s, z * 8 + y * 2 + c))
    return lax.ppermute(x, "sp", pairs)


def y_shift(x, by):
    return along_sp(x, lambda z, y, c: (z, (y + by) % 4, c))


def core_swap(x):
    return along_sp(x, lambda z, y, c: (z, y, 1 - c))


def tp_shift(x, by):
    return lax.ppermute(x, "tp", [(i, (i + by) % 4) for i in range(4)])


def dot(a, b):
    return jnp.dot(a, b, preferred_element_type=F32)


def project_kernel(t0, t1, t2, t3, gain, weights, qt, kv, scaled, inv_out):
    x = lax.axis_index("tp")
    squares = jnp.zeros((ROWS, 128), F32)
    for ref, by in zip((t0, t1, t2, t3), (0,) + SHIFTS):
        j = lax.rem(x - by + 4, 4)
        wide = ref[...].astype(F32)
        scaled[j] = (wide * gain[pl.ds(j, 1), :]).astype(BF16)
        sq = wide * wide
        squares += (sq[:, 0:128] + sq[:, 128:256]) + (sq[:, 256:384] + sq[:, 384:512])
    inv = lax.rsqrt(jnp.sum(squares, axis=1, keepdims=True) / D + EPSILON)
    inv_out[...] = jnp.broadcast_to(inv, (ROWS, 128))
    rows = jnp.concatenate([scaled[j] for j in range(4)], axis=1)
    both = dot(rows, weights[:, 256:512]) * inv
    k = both[:, 0:128].astype(BF16)
    vt = jnp.transpose(both[:, 128:256]).astype(BF16)
    for z in range(8):
        kv[z, 0:256, :] = k
        kv[z, 256:384, :] = vt[:, 0:128]
        kv[z, 384:512, :] = vt[:, 128:256]
    q = dot(rows, weights[:, 0:256]) * inv
    qt[...] = jnp.transpose(q * (QK ** -0.5)).astype(BF16)


def rest_kernel(scaled, inv_in, weights, glued, tail, gates):
    inv = inv_in[...]
    wide = jnp.concatenate([inv, inv], axis=1)
    rows = jnp.concatenate([scaled[j] for j in range(4)], axis=1)
    glu = (dot(rows, weights[:, 0:256]) * wide).astype(BF16).astype(F32)
    g = (glu[:, 0:128] * jax.nn.sigmoid(glu[:, 128:256])).astype(BF16)
    glued[...] = g
    tail[...] = g[ROWS - 32 :, :]
    gates[:, 128:384] = (dot(rows, weights[:, 256:512]) * wide).astype(BF16)
    gates[:, 0:128] = (dot(rows, weights[:, 512:640]) * inv).astype(BF16)


def conv_kernel(glued, before, weight, conv, squares, padded):
    padded[0:32, :] = before[...].astype(F32)
    padded[32 : 32 + ROWS, :] = glued[...].astype(F32)
    taps = weight[...].astype(F32)
    total = jnp.zeros((ROWS, 128), F32)
    for j in range(WIDTH):
        total += padded[j + 2 : j + 2 + ROWS, :] * taps[j : j + 1, :]
    conv[...] = total
    squares[...] = jnp.sum(jnp.transpose(total * total), axis=0, keepdims=True)


def attend(tiles, own, other, slot, queries, maxima, acc, mask=None):
    keys = jnp.concatenate([own[slot, 0:256, :], other[slot, 0:256, :]], axis=0)
    keys = jnp.concatenate([keys, keys], axis=1)
    values = jnp.concatenate(
        [
            own[slot, 256:384, :],
            own[slot, 384:512, :],
            other[slot, 256:384, :],
            other[slot, 384:512, :],
        ],
        axis=1,
    )
    values = jnp.concatenate([values, jnp.ones((ACC - VDIM, 512), BF16)], axis=0)
    ahead = [dot(keys, queries[t]) for t in tiles[:DEPTH]]
    for i, t in enumerate(tiles):
        scores = ahead.pop(0)
        if i + DEPTH < len(tiles):
            ahead.append(dot(keys, queries[tiles[i + DEPTH]]))
        if mask is not None:
            scores = jnp.where(mask, scores, NEG_BIG)
        old = maxima[t]
        new = jnp.maximum(old, jnp.max(scores, axis=0, keepdims=True))
        factor = jnp.exp2(old - new)
        expd = jnp.exp2(scores - new).astype(BF16)
        acc[t] = acc[t] * factor + dot(values, expd)
        maxima[t] = new


def lay_queries(q_refs, queries):
    none = jnp.zeros((64, ROWS), BF16)
    for b, ref in enumerate(q_refs):
        for t in range(4):
            g, m = t // 2, t % 2
            part = ref[g * 128 + m * 64 : g * 128 + m * 64 + 64, :].astype(F32) * LOG2E
            high = part.astype(BF16)
            low = (part - high.astype(F32)).astype(BF16)
            for i, rows in enumerate((high, low)):
                at = i * 128
                queries[b * 4 + t, at + m * 64 : at + m * 64 + 64, :] = rows
                queries[b * 4 + t, at + (1 - m) * 64 : at + (1 - m) * 64 + 64, :] = none


def write_part(out, first, maxima, acc):
    lines = []
    for t in range(4):
        i = first + t
        length = acc[i, VDIM : VDIM + 1, :]
        some = length > 0.0
        safe = jnp.where(some, length, 1.0)
        out[t * VDIM : (t + 1) * VDIM, :] = (acc[i, 0:VDIM, :] * (1.0 / safe)).astype(BF16)
        log = jnp.where(some, maxima[i] + jnp.log2(safe), NEG_BIG)
        for _ in range(3):
            piece = log.astype(BF16).astype(F32)
            lines.append(piece)
            log = log - piece
    lines.append(jnp.zeros((4, ROWS), F32))
    out[4 * VDIM : MSG, :] = jnp.concatenate(lines, axis=0).astype(BF16)


def position():
    s = lax.axis_index("sp")
    return s // 8, lax.rem(s // 2, 4), lax.rem(s, 2)


def start_state(maxima, acc):
    maxima[...] = jnp.full(maxima.shape, NEG_BIG, F32)
    acc[...] = jnp.zeros(acc.shape, F32)


def remote_kernel(q0, q1, q2, own, other, o0, o1, o2, queries, maxima, acc):
    z, y, _ = position()
    lay_queries((q0, q1, q2), queries)
    start_state(maxima, acc)

    def visit(i, carry):
        attend(range(12), own, other, i, queries, maxima, acc)
        return carry

    lax.fori_loop(0, z, visit, 0)
    for b, by in enumerate(SHIFTS):

        @pl.when(lax.rem(y - by + 4, 4) > y)
        def _(b=b):
            attend(range(4 * b, 4 * b + 4), own, other, z, queries, maxima, acc)

    for b, out in enumerate((o0, o1, o2)):
        write_part(out, 4 * b, maxima, acc)


def self_kernel(q0, own, other, out, queries, maxima, acc):
    z, _, c = position()
    lay_queries((q0,), queries)
    start_state(maxima, acc)
    row = lax.broadcasted_iota(jnp.int32, (512, ROWS), 0)
    key_row = jnp.where(row < ROWS, row + c * ROWS, row - c * ROWS)
    query_row = lax.broadcasted_iota(jnp.int32, (512, ROWS), 1) + c * ROWS
    attend(range(4), own, other, z, queries, maxima, acc, key_row <= query_row)

    def visit(i, carry):
        attend(range(4), own, other, i, queries, maxima, acc)
        return carry

    lax.fori_loop(0, z, visit, 0)
    write_part(out, 0, maxima, acc)


def merge_kernel(m0, m1, m2, m3, conv, s0, s1, s2, s3, c_gain, gates, lam, gain, y0, y1, y2, y3, rows):
    x = lax.axis_index("tp")
    total = (s0[...] + s1[...]) + (s2[...] + s3[...])
    inv = lax.rsqrt(total / CONV + EPSILON)
    inv = jnp.transpose(jnp.broadcast_to(inv, (128, ROWS)))
    normed = conv[...] * inv * c_gain[...]
    y_conv = (jax.nn.silu(normed) * jax.nn.silu(gates[:, 0:128].astype(F32))).astype(BF16)
    for j in range(4):
        rows[j, :, 0:128] = y_conv[64 * j : 64 * j + 64, :]
    logs = []
    for ref in (m0, m1, m2, m3):
        stats = ref[4 * VDIM : MSG, :].astype(F32)
        logs.append([(stats[3 * t : 3 * t + 1] + stats[3 * t + 1 : 3 * t + 2]) + stats[3 * t + 2 : 3 * t + 3] for t in range(4)])
    for g in range(2):
        maps = []
        for m in range(2):
            t = 2 * g + m
            top = functools.reduce(jnp.maximum, [l[t] for l in logs])
            weights = [jnp.exp2(l[t] - top) for l in logs]
            norm = 1.0 / functools.reduce(jnp.add, weights)
            part = [r[t * VDIM : (t + 1) * VDIM, :].astype(F32) * (w * norm) for r, w in zip((m0, m1, m2, m3), weights)]
            maps.append((part[0] + part[1]) + (part[2] + part[3]))
        o = maps[0] - lam[g] * maps[1]
        o = o * lax.rsqrt(jnp.mean(o * o, axis=0, keepdims=True) + EPSILON)
        o = jnp.transpose(o) * gain[...] * HEAD_SCALE
        gate = gates[:, 128 + g * 128 : 256 + g * 128].astype(F32)
        o = (o * jax.nn.silu(gate)).astype(BF16)
        for j in range(4):
            rows[j, :, 128 + g * 128 : 256 + g * 128] = o[64 * j : 64 * j + 64, :]
    for ref, by in zip((y0, y1, y2, y3), (0,) + SHIFTS):
        ref[...] = rows[lax.rem(x + by + 4, 4)]


def output_kernel(y0, y1, y2, y3, w_conv, w_attn, a1, a2, a3, b1, b2, b3, out):
    c = lax.rem(lax.axis_index("sp"), 2)
    y = y0[...]
    theirs = jnp.concatenate([y1[...], y2[...], y3[...]], axis=1)
    for half, refs in ((c, (a1, a2, a3)), (1 - c, (b1, b2, b3))):
        at = pl.ds(pl.multiple_of(half * 1024, 1024), 1024)
        mine = dot(y[:, 0:128], w_conv[:, at]) + dot(y[:, 128:384], w_attn[:, at])
        weights = jnp.concatenate([r[...] for r in refs], axis=0)
        out[:, at] = (mine + dot(theirs, weights)).astype(BF16)


def shape(dims, kind=BF16):
    return jax.ShapeDtypeStruct(dims, kind)


def sent(dims, kind=BF16):
    return pltpu.MemorySpace.HBM(dims, kind)


def local(
    tokens,
    in_gain,
    w_glu_value,
    w_glu_gate,
    w_query,
    w_key,
    w_value,
    w_gate_conv,
    w_gate_attn,
    conv_weight,
    conv_gain,
    lam,
    head_gain,
    out_conv,
    out_attn,
):
    c = lax.rem(lax.axis_index("sp"), 2)
    half = lax.dynamic_slice_in_dim(jnp.concatenate([out_conv, out_attn], axis=0), c * 1024, 1024, 1)
    pieces = [tokens] + [tp_shift(tokens, by) for by in SHIFTS]
    gain = in_gain.astype(F32).reshape(4, 512)
    first = jnp.concatenate([w_query, w_key, w_value], axis=1)
    second = jnp.concatenate([w_glu_value, w_glu_gate, w_gate_attn, w_gate_conv], axis=1)
    qt, kv, scaled, inv = pl.pallas_call(
        project_kernel,
        out_shape=[sent((256, ROWS)), sent((8, 512, 128)), shape((4, ROWS, 512)), shape((ROWS, 128), F32)],
        in_specs=[VM] * 6,
        out_specs=[OUT] * 2 + [VM] * 2,
        compiler_params=BIG,
        name="project",
    )(*pieces, gain, first)

    groups = [[z * 8 + r for z in range(8)] for r in range(8)]
    gathered = lax.all_to_all(kv, "sp", 0, 0, tiled=True, axis_index_groups=groups)
    q_blocks = [y_shift(qt, by) for by in SHIFTS]
    weights = [tp_shift(half, by) for by in SHIFTS]

    glued, tail, gates = pl.pallas_call(
        rest_kernel,
        out_shape=[shape((ROWS, 128)), sent((32, 128)), shape((ROWS, 384))],
        in_specs=[VM] * 3,
        out_specs=[VM, OUT, VM],
        compiler_params=BIG,
        name="rest",
    )(scaled, inv, second)
    before = lax.ppermute(tail, "sp", [(i, i + 1) for i in range(63)])
    conv, squares = pl.pallas_call(
        conv_kernel,
        out_shape=[shape((ROWS, 128), F32), sent((1, ROWS), F32)],
        in_specs=[VM] * 3,
        out_specs=[VM, OUT],
        scratch_shapes=[pltpu.VMEM((32 + ROWS, 128), F32)],
        name="conv",
    )(glued, before, conv_weight)
    sums = [squares] + [tp_shift(squares, by) for by in SHIFTS]

    swapped = core_swap(gathered)

    def scratch(tiles):
        return [
            pltpu.VMEM((tiles, 256, ROWS), BF16),
            pltpu.VMEM((tiles, 1, ROWS), F32),
            pltpu.VMEM((tiles, ACC, ROWS), F32),
        ]

    parts = pl.pallas_call(
        remote_kernel,
        out_shape=[sent((MSG, ROWS))] * 3,
        in_specs=[VM] * 5,
        out_specs=[OUT] * 3,
        scratch_shapes=scratch(12),
        compiler_params=BIG,
        name="remote",
    )(*q_blocks, gathered, swapped)
    back = [y_shift(part, -by) for part, by in zip(parts, SHIFTS)]
    parts, qt, weights = lax.optimization_barrier((parts, qt, weights))
    weights_s = [core_swap(w) for w in weights]
    part = pl.pallas_call(
        self_kernel,
        out_shape=shape((MSG, ROWS)),
        in_specs=[VM] * 3,
        out_specs=VM,
        scratch_shapes=scratch(4),
        compiler_params=BIG,
        name="self",
    )(qt, gathered, swapped)

    rows = pl.pallas_call(
        merge_kernel,
        out_shape=[shape((64, 384))] + [sent((64, 384))] * 3,
        in_specs=[VM] * 11 + [SM, VM],
        out_specs=[VM] + [OUT] * 3,
        scratch_shapes=[pltpu.VMEM((4, 64, 384), BF16)],
        compiler_params=BIG,
        name="merge",
    )(part, *back, conv, *sums, conv_gain.reshape(1, 128), gates, lam, head_gain.reshape(1, 128))
    rows = [rows[0]] + [tp_shift(r, by) for r, by in zip(rows[1:], SHIFTS)]
    return pl.pallas_call(
        output_kernel,
        out_shape=shape((64, D)),
        in_specs=[VM] * 12,
        out_specs=VM,
        compiler_params=BIG,
        name="output",
    )(*rows, out_conv, out_attn, *weights, *weights_s)


def solution(mesh):
    in_specs = (
        P("sp", "tp"),
        P(),
        P(None, "tp"),
        P(None, "tp"),
        P(None, "tp"),
        P(None, "tp"),
        P(None, "tp"),
        P(None, "tp"),
        P(None, "tp"),
        P(None, "tp"),
        P("tp"),
        P("tp"),
        P(),
        P("tp", None),
        P("tp", None),
    )
    out_specs = P(("sp", "tp"), None)

    return jax.shard_map(local, mesh=mesh, in_specs=in_specs, out_specs=out_specs, check_vma=False)
```

```python
import functools

import jax
import jax.numpy as jnp
from jax import lax
from jax.experimental import pallas as pl
from jax.experimental.pallas import tpu as pltpu
from jax.sharding import PartitionSpec as P


D = 2048
CONV = 512
QK = 64
VDIM = 128
WIDTH = 31
ROWS = 256
ACC = VDIM + 16
MSG = 4 * VDIM + 16

EPSILON = 1e-06
NEG_BIG = -1e30
HEAD_SCALE = 0.8


F32 = jnp.float32
BF16 = jnp.bfloat16
VM = pl.BlockSpec(memory_space=pltpu.VMEM)
OUT = pl.BlockSpec()
SM = pl.BlockSpec(memory_space=pltpu.SMEM)
ANY = pl.BlockSpec(memory_space=pltpu.MemorySpace.HBM)
BIG = pltpu.CompilerParams(vmem_limit_bytes=16 * 1024 * 1024)
SMALL = pltpu.CompilerParams(vmem_limit_bytes=8 * 1024 * 1024)
SHIFTS = (1, -1, 2)
DEPTH = 3
LOG2E = 1.4426950408889634


def place(s):
    return s // 8, (s // 2) % 4, s % 2


def along_sp(x, move):
    pairs = []
    for s in range(64):
        z, y, c = place(s)
        z, y, c = move(z, y, c)
        pairs.append((s, z * 8 + y * 2 + c))
    return lax.ppermute(x, "sp", pairs)


def y_shift(x, by):
    return along_sp(x, lambda z, y, c: (z, (y + by) % 4, c))


def core_swap(x):
    return along_sp(x, lambda z, y, c: (z, y, 1 - c))


def tp_shift(x, by):
    return lax.ppermute(x, "tp", [(i, (i + by) % 4) for i in range(4)])


def dot(a, b):
    return jnp.dot(a, b, preferred_element_type=F32)


def project_kernel(t0, t1, t2, t3, gain, weights, qt, kv, scaled, inv_out):
    x = lax.axis_index("tp")
    squares = jnp.zeros((ROWS, 128), F32)
    for ref, by in zip((t0, t1, t2, t3), (0,) + SHIFTS):
        j = lax.rem(x - by + 4, 4)
        wide = ref[...].astype(F32)
        scaled[j] = (wide * gain[pl.ds(j, 1), :]).astype(BF16)
        sq = wide * wide
        squares += (sq[:, 0:128] + sq[:, 128:256]) + (sq[:, 256:384] + sq[:, 384:512])
    inv = lax.rsqrt(jnp.sum(squares, axis=1, keepdims=True) / D + EPSILON)
    inv_out[...] = jnp.broadcast_to(inv, (ROWS, 128))
    rows = jnp.concatenate([scaled[j] for j in range(4)], axis=1)
    both = dot(rows, weights[:, 256:512]) * inv
    k = both[:, 0:128].astype(BF16)
    vt = jnp.transpose(both[:, 128:256]).astype(BF16)
    for z in range(8):
        kv[z, 0:256, :] = k
        kv[z, 256:384, :] = vt[:, 0:128]
        kv[z, 384:512, :] = vt[:, 128:256]
    q = dot(rows, weights[:, 0:256]) * inv
    qt[...] = jnp.transpose(q * (QK ** -0.5)).astype(BF16)


def rest_kernel(scaled, inv_in, weights, glued, tail, gates):
    inv = inv_in[...]
    wide = jnp.concatenate([inv, inv], axis=1)
    rows = jnp.concatenate([scaled[j] for j in range(4)], axis=1)
    glu = (dot(rows, weights[:, 0:256]) * wide).astype(BF16).astype(F32)
    g = (glu[:, 0:128] * jax.nn.sigmoid(glu[:, 128:256])).astype(BF16)
    glued[...] = g
    tail[...] = g[ROWS - 32 :, :]
    gates[:, 128:384] = (dot(rows, weights[:, 256:512]) * wide).astype(BF16)
    gates[:, 0:128] = (dot(rows, weights[:, 512:640]) * inv).astype(BF16)


def conv_kernel(glued, before, weight, conv, squares, padded):
    padded[0:32, :] = before[...].astype(F32)
    padded[32 : 32 + ROWS, :] = glued[...].astype(F32)
    taps = weight[...].astype(F32)
    total = jnp.zeros((ROWS, 128), F32)
    for j in range(WIDTH):
        total += padded[j + 2 : j + 2 + ROWS, :] * taps[j : j + 1, :]
    conv[...] = total
    squares[...] = jnp.sum(jnp.transpose(total * total), axis=0, keepdims=True)


def attend(tiles, own, other, slot, queries, maxima, acc, mask=None):
    keys = jnp.concatenate([own[slot, 0:256, :], other[slot, 0:256, :]], axis=0)
    keys = jnp.concatenate([keys, keys], axis=1)
    values = jnp.concatenate(
        [
            own[slot, 256:384, :],
            own[slot, 384:512, :],
            other[slot, 256:384, :],
            other[slot, 384:512, :],
        ],
        axis=1,
    )
    values = jnp.concatenate([values, jnp.ones((ACC - VDIM, 512), BF16)], axis=0)
    ahead = [dot(keys, queries[t]) for t in tiles[:DEPTH]]
    for i, t in enumerate(tiles):
        scores = ahead.pop(0)
        if i + DEPTH < len(tiles):
            ahead.append(dot(keys, queries[tiles[i + DEPTH]]))
        if mask is not None:
            scores = jnp.where(mask, scores, NEG_BIG)
        old = maxima[t]
        new = jnp.maximum(old, jnp.max(scores, axis=0, keepdims=True))
        factor = jnp.exp2(old - new)
        expd = jnp.exp2(scores - new).astype(BF16)
        acc[t] = acc[t] * factor + dot(values, expd)
        maxima[t] = new


def lay_queries(q_refs, queries):
    none = jnp.zeros((64, ROWS), BF16)
    for b, ref in enumerate(q_refs):
        for t in range(4):
            g, m = t // 2, t % 2
            part = ref[g * 128 + m * 64 : g * 128 + m * 64 + 64, :].astype(F32) * LOG2E
            high = part.astype(BF16)
            low = (part - high.astype(F32)).astype(BF16)
            for i, rows in enumerate((high, low)):
                at = i * 128
                queries[b * 4 + t, at + m * 64 : at + m * 64 + 64, :] = rows
                queries[b * 4 + t, at + (1 - m) * 64 : at + (1 - m) * 64 + 64, :] = none


def write_part(out, first, maxima, acc):
    lines = []
    for t in range(4):
        i = first + t
        length = acc[i, VDIM : VDIM + 1, :]
        some = length > 0.0
        safe = jnp.where(some, length, 1.0)
        out[t * VDIM : (t + 1) * VDIM, :] = (acc[i, 0:VDIM, :] * (1.0 / safe)).astype(BF16)
        log = jnp.where(some, maxima[i] + jnp.log2(safe), NEG_BIG)
        for _ in range(3):
            piece = log.astype(BF16).astype(F32)
            lines.append(piece)
            log = log - piece
    lines.append(jnp.zeros((4, ROWS), F32))
    out[4 * VDIM : MSG, :] = jnp.concatenate(lines, axis=0).astype(BF16)


def position():
    s = lax.axis_index("sp")
    return s // 8, lax.rem(s // 2, 4), lax.rem(s, 2)


def start_state(maxima, acc):
    maxima[...] = jnp.full(maxima.shape, NEG_BIG, F32)
    acc[...] = jnp.zeros(acc.shape, F32)


def remote_kernel(q0, q1, q2, own, other, o0, o1, o2, queries, maxima, acc):
    z, y, _ = position()
    lay_queries((q0, q1, q2), queries)
    start_state(maxima, acc)

    def visit(i, carry):
        attend(range(12), own, other, i, queries, maxima, acc)
        return carry

    lax.fori_loop(0, z, visit, 0)
    for b, by in enumerate(SHIFTS):

        @pl.when(lax.rem(y - by + 4, 4) > y)
        def _(b=b):
            attend(range(4 * b, 4 * b + 4), own, other, z, queries, maxima, acc)

    for b, out in enumerate((o0, o1, o2)):
        write_part(out, 4 * b, maxima, acc)


def self_kernel(q0, own, other, out, queries, maxima, acc):
    z, _, c = position()
    lay_queries((q0,), queries)
    start_state(maxima, acc)
    row = lax.broadcasted_iota(jnp.int32, (512, ROWS), 0)
    key_row = jnp.where(row < ROWS, row + c * ROWS, row - c * ROWS)
    query_row = lax.broadcasted_iota(jnp.int32, (512, ROWS), 1) + c * ROWS
    attend(range(4), own, other, z, queries, maxima, acc, key_row <= query_row)

    def visit(i, carry):
        attend(range(4), own, other, i, queries, maxima, acc)
        return carry

    lax.fori_loop(0, z, visit, 0)
    write_part(out, 0, maxima, acc)


def merge_kernel(m0, m1, m2, m3, conv, s0, s1, s2, s3, c_gain, gates, lam, gain, y0, y1, y2, y3, rows):
    x = lax.axis_index("tp")
    total = (s0[...] + s1[...]) + (s2[...] + s3[...])
    inv = lax.rsqrt(total / CONV + EPSILON)
    inv = jnp.transpose(jnp.broadcast_to(inv, (128, ROWS)))
    normed = conv[...] * inv * c_gain[...]
    y_conv = (jax.nn.silu(normed) * jax.nn.silu(gates[:, 0:128].astype(F32))).astype(BF16)
    for j in range(4):
        rows[j, :, 0:128] = y_conv[64 * j : 64 * j + 64, :]
    logs = []
    for ref in (m0, m1, m2, m3):
        stats = ref[4 * VDIM : MSG, :].astype(F32)
        logs.append([(stats[3 * t : 3 * t + 1] + stats[3 * t + 1 : 3 * t + 2]) + stats[3 * t + 2 : 3 * t + 3] for t in range(4)])
    for g in range(2):
        maps = []
        for m in range(2):
            t = 2 * g + m
            top = functools.reduce(jnp.maximum, [l[t] for l in logs])
            weights = [jnp.exp2(l[t] - top) for l in logs]
            norm = 1.0 / functools.reduce(jnp.add, weights)
            part = [r[t * VDIM : (t + 1) * VDIM, :].astype(F32) * (w * norm) for r, w in zip((m0, m1, m2, m3), weights)]
            maps.append((part[0] + part[1]) + (part[2] + part[3]))
        o = maps[0] - lam[g] * maps[1]
        o = o * lax.rsqrt(jnp.mean(o * o, axis=0, keepdims=True) + EPSILON)
        o = jnp.transpose(o) * gain[...] * HEAD_SCALE
        gate = gates[:, 128 + g * 128 : 256 + g * 128].astype(F32)
        o = (o * jax.nn.silu(gate)).astype(BF16)
        for j in range(4):
            rows[j, :, 128 + g * 128 : 256 + g * 128] = o[64 * j : 64 * j + 64, :]
    for ref, by in zip((y0, y1, y2, y3), (0,) + SHIFTS):
        ref[...] = rows[lax.rem(x + by + 4, 4)]


def output_kernel(y0, y1, y2, y3, w_conv, w_attn, a1, a2, a3, b1, b2, b3, out):
    c = lax.rem(lax.axis_index("sp"), 2)
    y = y0[...]
    theirs = jnp.concatenate([y1[...], y2[...], y3[...]], axis=1)
    for half, refs in ((c, (a1, a2, a3)), (1 - c, (b1, b2, b3))):
        at = pl.ds(pl.multiple_of(half * 1024, 1024), 1024)
        mine = dot(y[:, 0:128], w_conv[:, at]) + dot(y[:, 128:384], w_attn[:, at])
        weights = jnp.concatenate([r[...] for r in refs], axis=0)
        out[:, at] = (mine + dot(theirs, weights)).astype(BF16)


def shape(dims, kind=BF16):
    return jax.ShapeDtypeStruct(dims, kind)


def sent(dims, kind=BF16):
    return pltpu.MemorySpace.HBM(dims, kind)


def local(
    tokens,
    in_gain,
    w_glu_value,
    w_glu_gate,
    w_query,
    w_key,
    w_value,
    w_gate_conv,
    w_gate_attn,
    conv_weight,
    conv_gain,
    lam,
    head_gain,
    out_conv,
    out_attn,
):
    c = lax.rem(lax.axis_index("sp"), 2)
    half = lax.dynamic_slice_in_dim(jnp.concatenate([out_conv, out_attn], axis=0), c * 1024, 1024, 1)
    pieces = [tokens] + [tp_shift(tokens, by) for by in SHIFTS]
    gain = in_gain.astype(F32).reshape(4, 512)
    first = jnp.concatenate([w_query, w_key, w_value], axis=1)
    second = jnp.concatenate([w_glu_value, w_glu_gate, w_gate_attn, w_gate_conv], axis=1)
    gain, first, second, half = lax.optimization_barrier((gain, first, second, half))
    qt, kv, scaled, inv = pl.pallas_call(
        project_kernel,
        out_shape=[sent((256, ROWS)), sent((8, 512, 128)), sent((4, ROWS, 512)), sent((ROWS, 128), F32)],
        in_specs=[VM] * 6,
        out_specs=[OUT] * 4,
        compiler_params=SMALL,
        name="project",
    )(*pieces, gain, first)

    groups = [[z * 8 + r for z in range(8)] for r in range(8)]
    gathered = lax.all_to_all(kv, "sp", 0, 0, tiled=True, axis_index_groups=groups)
    q_blocks = [y_shift(qt, by) for by in SHIFTS]
    weights = [tp_shift(half, by) for by in SHIFTS]

    glued, tail, gates = pl.pallas_call(
        rest_kernel,
        out_shape=[shape((ROWS, 128)), sent((32, 128)), shape((ROWS, 384))],
        in_specs=[VM] * 3,
        out_specs=[VM, OUT, VM],
        compiler_params=SMALL,
        name="rest",
    )(scaled, inv, second)
    before = lax.ppermute(tail, "sp", [(i, i + 1) for i in range(63)])
    conv, squares = pl.pallas_call(
        conv_kernel,
        out_shape=[sent((ROWS, 128), F32), sent((1, ROWS), F32)],
        in_specs=[VM] * 3,
        out_specs=[OUT] * 2,
        scratch_shapes=[pltpu.VMEM((32 + ROWS, 128), F32)],
        compiler_params=SMALL,
        name="conv",
    )(glued, before, conv_weight)
    sums = [squares] + [tp_shift(squares, by) for by in SHIFTS]

    swapped = core_swap(gathered)

    def scratch(tiles):
        return [
            pltpu.VMEM((tiles, 256, ROWS), BF16),
            pltpu.VMEM((tiles, 1, ROWS), F32),
            pltpu.VMEM((tiles, ACC, ROWS), F32),
        ]

    parts = pl.pallas_call(
        remote_kernel,
        out_shape=[sent((MSG, ROWS))] * 3,
        in_specs=[VM] * 5,
        out_specs=[OUT] * 3,
        scratch_shapes=scratch(12),
        compiler_params=BIG,
        name="remote",
    )(*q_blocks, gathered, swapped)
    back = [y_shift(part, -by) for part, by in zip(parts, SHIFTS)]
    parts, qt, weights = lax.optimization_barrier((parts, qt, weights))
    weights_s = [core_swap(w) for w in weights]
    part = pl.pallas_call(
        self_kernel,
        out_shape=shape((MSG, ROWS)),
        in_specs=[VM] * 3,
        out_specs=VM,
        scratch_shapes=scratch(4),
        compiler_params=BIG,
        name="self",
    )(qt, gathered, swapped)

    rows = pl.pallas_call(
        merge_kernel,
        out_shape=[shape((64, 384))] + [sent((64, 384))] * 3,
        in_specs=[VM] * 11 + [SM, VM],
        out_specs=[VM] + [OUT] * 3,
        scratch_shapes=[pltpu.VMEM((4, 64, 384), BF16)],
        compiler_params=SMALL,
        name="merge",
    )(part, *back, conv, *sums, conv_gain.reshape(1, 128), gates, lam, head_gain.reshape(1, 128))
    rows = [rows[0]] + [tp_shift(r, by) for r, by in zip(rows[1:], SHIFTS)]
    return pl.pallas_call(
        output_kernel,
        out_shape=shape((64, D)),
        in_specs=[VM] * 12,
        out_specs=VM,
        compiler_params=BIG,
        name="output",
    )(*rows, out_conv, out_attn, *weights, *weights_s)


def solution(mesh):
    in_specs = (
        P("sp", "tp"),
        P(),
        P(None, "tp"),
        P(None, "tp"),
        P(None, "tp"),
        P(None, "tp"),
        P(None, "tp"),
        P(None, "tp"),
        P(None, "tp"),
        P(None, "tp"),
        P("tp"),
        P("tp"),
        P(),
        P("tp", None),
        P("tp", None),
    )
    out_specs = P(("sp", "tp"), None)

    return jax.shard_map(local, mesh=mesh, in_specs=in_specs, out_specs=out_specs, check_vma=False)
```

```python
import functools

import jax
import jax.numpy as jnp
from jax import lax
from jax.experimental import pallas as pl
from jax.experimental.pallas import tpu as pltpu
from jax.sharding import PartitionSpec as P


D = 2048
CONV = 512
QK = 64
VDIM = 128
WIDTH = 31
ROWS = 256
ACC = VDIM + 16
MSG = 4 * VDIM + 16

EPSILON = 1e-06
NEG_BIG = -1e30
HEAD_SCALE = 0.8


F32 = jnp.float32
BF16 = jnp.bfloat16
VM = pl.BlockSpec(memory_space=pltpu.VMEM)
OUT = pl.BlockSpec()
SM = pl.BlockSpec(memory_space=pltpu.SMEM)
ANY = pl.BlockSpec(memory_space=pltpu.MemorySpace.HBM)
BIG = pltpu.CompilerParams(vmem_limit_bytes=16 * 1024 * 1024)
SMALL = pltpu.CompilerParams(vmem_limit_bytes=8 * 1024 * 1024)
SHIFTS = (1, -1, 2)
DEPTH = 3
LOG2E = 1.4426950408889634


def place(s):
    return s // 8, (s // 2) % 4, s % 2


def along_sp(x, move):
    pairs = []
    for s in range(64):
        z, y, c = place(s)
        z, y, c = move(z, y, c)
        pairs.append((s, z * 8 + y * 2 + c))
    return lax.ppermute(x, "sp", pairs)


def y_shift(x, by):
    return along_sp(x, lambda z, y, c: (z, (y + by) % 4, c))


def core_swap(x):
    return along_sp(x, lambda z, y, c: (z, y, 1 - c))


def tp_shift(x, by):
    return lax.ppermute(x, "tp", [(i, (i + by) % 4) for i in range(4)])


def dot(a, b):
    return jnp.dot(a, b, preferred_element_type=F32)


def project_kernel(t0, t1, t2, t3, gain, weights, qt, kv, scaled, inv_out):
    x = lax.axis_index("tp")
    squares = jnp.zeros((ROWS, 128), F32)
    for ref, by in zip((t0, t1, t2, t3), (0,) + SHIFTS):
        j = lax.rem(x - by + 4, 4)
        wide = ref[...].astype(F32)
        scaled[j] = (wide * gain[pl.ds(j, 1), :]).astype(BF16)
        sq = wide * wide
        squares += (sq[:, 0:128] + sq[:, 128:256]) + (sq[:, 256:384] + sq[:, 384:512])
    inv = lax.rsqrt(jnp.sum(squares, axis=1, keepdims=True) / D + EPSILON)
    inv_out[...] = jnp.broadcast_to(inv, (ROWS, 128))
    rows = jnp.concatenate([scaled[j] for j in range(4)], axis=1)
    both = dot(rows, weights[:, 256:512]) * inv
    k = both[:, 0:128].astype(BF16)
    vt = jnp.transpose(both[:, 128:256]).astype(BF16)
    for z in range(8):
        kv[z, 0:256, :] = k
        kv[z, 256:384, :] = vt[:, 0:128]
        kv[z, 384:512, :] = vt[:, 128:256]
    q = dot(rows, weights[:, 0:256]) * inv
    qt[...] = jnp.transpose(q * (QK ** -0.5)).astype(BF16)


def rest_kernel(scaled, inv_in, weights, glued, tail, gates):
    inv = inv_in[...]
    wide = jnp.concatenate([inv, inv], axis=1)
    rows = jnp.concatenate([scaled[j] for j in range(4)], axis=1)
    glu = (dot(rows, weights[:, 0:256]) * wide).astype(BF16).astype(F32)
    g = (glu[:, 0:128] * jax.nn.sigmoid(glu[:, 128:256])).astype(BF16)
    glued[...] = g
    tail[...] = g[ROWS - 32 :, :]
    gates[:, 128:384] = (dot(rows, weights[:, 256:512]) * wide).astype(BF16)
    gates[:, 0:128] = (dot(rows, weights[:, 512:640]) * inv).astype(BF16)


def conv_kernel(glued, before, weight, conv, squares, kept, padded):
    padded[0:32, :] = before[...].astype(F32)
    padded[32 : 32 + ROWS, :] = glued[...].astype(F32)
    taps = weight[...].astype(F32)
    total = jnp.zeros((ROWS, 128), F32)
    for j in range(WIDTH):
        total += padded[j + 2 : j + 2 + ROWS, :] * taps[j : j + 1, :]
    conv[...] = total
    sums = jnp.sum(jnp.transpose(total * total), axis=0, keepdims=True)
    squares[...] = sums
    kept[...] = sums


def attend(tiles, own, other, slot, queries, maxima, acc, mask=None):
    keys = jnp.concatenate([own[slot, 0:256, :], other[slot, 0:256, :]], axis=0)
    keys = jnp.concatenate([keys, keys], axis=1)
    values = jnp.concatenate(
        [
            own[slot, 256:384, :],
            own[slot, 384:512, :],
            other[slot, 256:384, :],
            other[slot, 384:512, :],
        ],
        axis=1,
    )
    values = jnp.concatenate([values, jnp.ones((ACC - VDIM, 512), BF16)], axis=0)
    ahead = [dot(keys, queries[t]) for t in tiles[:DEPTH]]
    for i, t in enumerate(tiles):
        scores = ahead.pop(0)
        if i + DEPTH < len(tiles):
            ahead.append(dot(keys, queries[tiles[i + DEPTH]]))
        if mask is not None:
            scores = jnp.where(mask, scores, NEG_BIG)
        old = maxima[t]
        new = jnp.maximum(old, jnp.max(scores, axis=0, keepdims=True))
        factor = jnp.exp2(old - new)
        expd = jnp.exp2(scores - new).astype(BF16)
        acc[t] = acc[t] * factor + dot(values, expd)
        maxima[t] = new


def lay_queries(q_refs, queries):
    none = jnp.zeros((64, ROWS), BF16)
    for b, ref in enumerate(q_refs):
        for t in range(4):
            g, m = t // 2, t % 2
            part = ref[g * 128 + m * 64 : g * 128 + m * 64 + 64, :].astype(F32) * LOG2E
            high = part.astype(BF16)
            low = (part - high.astype(F32)).astype(BF16)
            for i, rows in enumerate((high, low)):
                at = i * 128
                queries[b * 4 + t, at + m * 64 : at + m * 64 + 64, :] = rows
                queries[b * 4 + t, at + (1 - m) * 64 : at + (1 - m) * 64 + 64, :] = none


def write_part(out, first, maxima, acc):
    lines = []
    for t in range(4):
        i = first + t
        length = acc[i, VDIM : VDIM + 1, :]
        some = length > 0.0
        safe = jnp.where(some, length, 1.0)
        out[t * VDIM : (t + 1) * VDIM, :] = (acc[i, 0:VDIM, :] * (1.0 / safe)).astype(BF16)
        log = jnp.where(some, maxima[i] + jnp.log2(safe), NEG_BIG)
        for _ in range(3):
            piece = log.astype(BF16).astype(F32)
            lines.append(piece)
            log = log - piece
    lines.append(jnp.zeros((4, ROWS), F32))
    out[4 * VDIM : MSG, :] = jnp.concatenate(lines, axis=0).astype(BF16)


def position():
    s = lax.axis_index("sp")
    return s // 8, lax.rem(s // 2, 4), lax.rem(s, 2)


def start_state(maxima, acc):
    maxima[...] = jnp.full(maxima.shape, NEG_BIG, F32)
    acc[...] = jnp.zeros(acc.shape, F32)


def remote_kernel(q0, q1, q2, own, other, o0, o1, o2, queries, maxima, acc):
    z, y, _ = position()
    lay_queries((q0, q1, q2), queries)
    start_state(maxima, acc)

    def visit(i, carry):
        attend(range(12), own, other, i, queries, maxima, acc)
        return carry

    lax.fori_loop(0, z, visit, 0)
    for b, by in enumerate(SHIFTS):

        @pl.when(lax.rem(y - by + 4, 4) > y)
        def _(b=b):
            attend(range(4 * b, 4 * b + 4), own, other, z, queries, maxima, acc)

    for b, out in enumerate((o0, o1, o2)):
        write_part(out, 4 * b, maxima, acc)


def self_kernel(q0, own, other, out, queries, maxima, acc):
    z, _, c = position()
    lay_queries((q0,), queries)
    start_state(maxima, acc)
    row = lax.broadcasted_iota(jnp.int32, (512, ROWS), 0)
    key_row = jnp.where(row < ROWS, row + c * ROWS, row - c * ROWS)
    query_row = lax.broadcasted_iota(jnp.int32, (512, ROWS), 1) + c * ROWS
    attend(range(4), own, other, z, queries, maxima, acc, key_row <= query_row)

    def visit(i, carry):
        attend(range(4), own, other, i, queries, maxima, acc)
        return carry

    lax.fori_loop(0, z, visit, 0)
    write_part(out, 0, maxima, acc)


def merge_kernel(m0, m1, m2, m3, conv, s0, s1, s2, s3, c_gain, gates, lam, gain, y0, y1, y2, y3, rows):
    x = lax.axis_index("tp")
    total = (s0[...] + s1[...]) + (s2[...] + s3[...])
    inv = lax.rsqrt(total / CONV + EPSILON)
    inv = jnp.transpose(jnp.broadcast_to(inv, (128, ROWS)))
    normed = conv[...] * inv * c_gain[...]
    y_conv = (jax.nn.silu(normed) * jax.nn.silu(gates[:, 0:128].astype(F32))).astype(BF16)
    for j in range(4):
        rows[j, :, 0:128] = y_conv[64 * j : 64 * j + 64, :]
    logs = []
    for ref in (m0, m1, m2, m3):
        stats = ref[4 * VDIM : MSG, :].astype(F32)
        logs.append([(stats[3 * t : 3 * t + 1] + stats[3 * t + 1 : 3 * t + 2]) + stats[3 * t + 2 : 3 * t + 3] for t in range(4)])
    for g in range(2):
        maps = []
        for m in range(2):
            t = 2 * g + m
            top = functools.reduce(jnp.maximum, [l[t] for l in logs])
            weights = [jnp.exp2(l[t] - top) for l in logs]
            norm = 1.0 / functools.reduce(jnp.add, weights)
            part = [r[t * VDIM : (t + 1) * VDIM, :].astype(F32) * (w * norm) for r, w in zip((m0, m1, m2, m3), weights)]
            maps.append((part[0] + part[1]) + (part[2] + part[3]))
        o = maps[0] - lam[g] * maps[1]
        o = o * lax.rsqrt(jnp.mean(o * o, axis=0, keepdims=True) + EPSILON)
        o = jnp.transpose(o) * gain[...] * HEAD_SCALE
        gate = gates[:, 128 + g * 128 : 256 + g * 128].astype(F32)
        o = (o * jax.nn.silu(gate)).astype(BF16)
        for j in range(4):
            rows[j, :, 128 + g * 128 : 256 + g * 128] = o[64 * j : 64 * j + 64, :]
    for ref, by in zip((y0, y1, y2, y3), (0,) + SHIFTS):
        ref[...] = rows[lax.rem(x + by + 4, 4)]


def output_kernel(y0, y1, y2, y3, w_conv, w_attn, a1, a2, a3, b1, b2, b3, out):
    c = lax.rem(lax.axis_index("sp"), 2)
    y = y0[...]
    theirs = jnp.concatenate([y1[...], y2[...], y3[...]], axis=1)
    for half, refs in ((c, (a1, a2, a3)), (1 - c, (b1, b2, b3))):
        at = pl.ds(pl.multiple_of(half * 1024, 1024), 1024)
        mine = dot(y[:, 0:128], w_conv[:, at]) + dot(y[:, 128:384], w_attn[:, at])
        weights = jnp.concatenate([r[...] for r in refs], axis=0)
        out[:, at] = (mine + dot(theirs, weights)).astype(BF16)


def shape(dims, kind=BF16):
    return jax.ShapeDtypeStruct(dims, kind)


def sent(dims, kind=BF16):
    return pltpu.MemorySpace.HBM(dims, kind)


def local(
    tokens,
    in_gain,
    w_glu_value,
    w_glu_gate,
    w_query,
    w_key,
    w_value,
    w_gate_conv,
    w_gate_attn,
    conv_weight,
    conv_gain,
    lam,
    head_gain,
    out_conv,
    out_attn,
):
    c = lax.rem(lax.axis_index("sp"), 2)
    half = lax.dynamic_slice_in_dim(jnp.concatenate([out_conv, out_attn], axis=0), c * 1024, 1024, 1)
    pieces = [tokens] + [tp_shift(tokens, by) for by in SHIFTS]
    gain = in_gain.astype(F32).reshape(4, 512)
    first = jnp.concatenate([w_query, w_key, w_value], axis=1)
    second = jnp.concatenate([w_glu_value, w_glu_gate, w_gate_attn, w_gate_conv], axis=1)
    gain, first, second, half = lax.optimization_barrier((gain, first, second, half))
    qt, kv, scaled, inv = pl.pallas_call(
        project_kernel,
        out_shape=[sent((256, ROWS)), sent((8, 512, 128)), sent((4, ROWS, 512)), sent((ROWS, 128), F32)],
        in_specs=[VM] * 6,
        out_specs=[OUT] * 4,
        compiler_params=SMALL,
        name="project",
    )(*pieces, gain, first)

    groups = [[z * 8 + r for z in range(8)] for r in range(8)]
    gathered = lax.all_to_all(kv, "sp", 0, 0, tiled=True, axis_index_groups=groups)
    q_blocks = [y_shift(qt, by) for by in SHIFTS]
    weights = [tp_shift(half, by) for by in SHIFTS]

    glued, tail, gates = pl.pallas_call(
        rest_kernel,
        out_shape=[shape((ROWS, 128)), sent((32, 128)), shape((ROWS, 384))],
        in_specs=[VM] * 3,
        out_specs=[VM, OUT, VM],
        compiler_params=SMALL,
        name="rest",
    )(scaled, inv, second)
    before = lax.ppermute(tail, "sp", [(i, i + 1) for i in range(63)])
    conv, squares, kept = pl.pallas_call(
        conv_kernel,
        out_shape=[shape((ROWS, 128), F32), sent((1, ROWS), F32), shape((1, ROWS), F32)],
        in_specs=[VM] * 3,
        out_specs=[VM, OUT, VM],
        scratch_shapes=[pltpu.VMEM((32 + ROWS, 128), F32)],
        compiler_params=SMALL,
        name="conv",
    )(glued, before, conv_weight)
    sums = [kept] + [tp_shift(squares, by) for by in SHIFTS]

    swapped = core_swap(gathered)

    def scratch(tiles):
        return [
            pltpu.VMEM((tiles, 256, ROWS), BF16),
            pltpu.VMEM((tiles, 1, ROWS), F32),
            pltpu.VMEM((tiles, ACC, ROWS), F32),
        ]

    parts = pl.pallas_call(
        remote_kernel,
        out_shape=[sent((MSG, ROWS))] * 3,
        in_specs=[VM] * 5,
        out_specs=[OUT] * 3,
        scratch_shapes=scratch(12),
        compiler_params=BIG,
        name="remote",
    )(*q_blocks, gathered, swapped)
    back = [y_shift(part, -by) for part, by in zip(parts, SHIFTS)]
    parts, qt, weights = lax.optimization_barrier((parts, qt, weights))
    weights_s = [core_swap(w) for w in weights]
    part = pl.pallas_call(
        self_kernel,
        out_shape=shape((MSG, ROWS)),
        in_specs=[VM] * 3,
        out_specs=VM,
        scratch_shapes=scratch(4),
        compiler_params=BIG,
        name="self",
    )(qt, gathered, swapped)

    rows = pl.pallas_call(
        merge_kernel,
        out_shape=[shape((64, 384))] + [sent((64, 384))] * 3,
        in_specs=[VM] * 11 + [SM, VM],
        out_specs=[VM] + [OUT] * 3,
        scratch_shapes=[pltpu.VMEM((4, 64, 384), BF16)],
        compiler_params=SMALL,
        name="merge",
    )(part, *back, conv, *sums, conv_gain.reshape(1, 128), gates, lam, head_gain.reshape(1, 128))
    rows = [rows[0]] + [tp_shift(r, by) for r, by in zip(rows[1:], SHIFTS)]
    return pl.pallas_call(
        output_kernel,
        out_shape=shape((64, D)),
        in_specs=[VM] * 12,
        out_specs=VM,
        compiler_params=BIG,
        name="output",
    )(*rows, out_conv, out_attn, *weights, *weights_s)


def solution(mesh):
    in_specs = (
        P("sp", "tp"),
        P(),
        P(None, "tp"),
        P(None, "tp"),
        P(None, "tp"),
        P(None, "tp"),
        P(None, "tp"),
        P(None, "tp"),
        P(None, "tp"),
        P(None, "tp"),
        P("tp"),
        P("tp"),
        P(),
        P("tp", None),
        P("tp", None),
    )
    out_specs = P(("sp", "tp"), None)

    return jax.shard_map(local, mesh=mesh, in_specs=in_specs, out_specs=out_specs, check_vma=False)
```

```python
import functools

import jax
import jax.numpy as jnp
from jax import lax
from jax.experimental import pallas as pl
from jax.experimental.pallas import tpu as pltpu
from jax.sharding import PartitionSpec as P


D = 2048
CONV = 512
QK = 64
VDIM = 128
WIDTH = 31
ROWS = 256
ACC = VDIM + 16
MSG = 4 * VDIM + 16

EPSILON = 1e-06
NEG_BIG = -1e30
HEAD_SCALE = 0.8


F32 = jnp.float32
BF16 = jnp.bfloat16
VM = pl.BlockSpec(memory_space=pltpu.VMEM)
OUT = pl.BlockSpec()
SM = pl.BlockSpec(memory_space=pltpu.SMEM)
ANY = pl.BlockSpec(memory_space=pltpu.MemorySpace.HBM)
BIG = pltpu.CompilerParams(vmem_limit_bytes=16 * 1024 * 1024)
SMALL = pltpu.CompilerParams(vmem_limit_bytes=8 * 1024 * 1024)
SHIFTS = (1, -1, 2)
DEPTH = 3
LOG2E = 1.4426950408889634


def place(s):
    return s // 8, (s // 2) % 4, s % 2


def along_sp(x, move):
    pairs = []
    for s in range(64):
        z, y, c = place(s)
        z, y, c = move(z, y, c)
        pairs.append((s, z * 8 + y * 2 + c))
    return lax.ppermute(x, "sp", pairs)


def y_shift(x, by):
    return along_sp(x, lambda z, y, c: (z, (y + by) % 4, c))


def core_swap(x):
    return along_sp(x, lambda z, y, c: (z, y, 1 - c))


def tp_shift(x, by):
    return lax.ppermute(x, "tp", [(i, (i + by) % 4) for i in range(4)])


def dot(a, b):
    return jnp.dot(a, b, preferred_element_type=F32)


def project_kernel(t0, t1, t2, t3, gain, weights, qt, kv, scaled, inv_out):
    x = lax.axis_index("tp")
    squares = jnp.zeros((ROWS, 128), F32)
    for ref, by in zip((t0, t1, t2, t3), (0,) + SHIFTS):
        j = lax.rem(x - by + 4, 4)
        wide = ref[...].astype(F32)
        scaled[j] = (wide * gain[pl.ds(j, 1), :]).astype(BF16)
        sq = wide * wide
        squares += (sq[:, 0:128] + sq[:, 128:256]) + (sq[:, 256:384] + sq[:, 384:512])
    inv = lax.rsqrt(jnp.sum(squares, axis=1, keepdims=True) / D + EPSILON)
    inv_out[...] = jnp.broadcast_to(inv, (ROWS, 128))
    rows = jnp.concatenate([scaled[j] for j in range(4)], axis=1)
    both = dot(rows, weights[:, 256:512]) * inv
    k = both[:, 0:128].astype(BF16)
    vt = jnp.transpose(both[:, 128:256]).astype(BF16)
    for z in range(8):
        kv[z, 0:256, :] = k
        kv[z, 256:384, :] = vt[:, 0:128]
        kv[z, 384:512, :] = vt[:, 128:256]
    q = dot(rows, weights[:, 0:256]) * inv
    qt[...] = jnp.transpose(q * (QK ** -0.5)).astype(BF16)


def rest_kernel(scaled, inv_in, weights, glued, tail, gates):
    inv = inv_in[...]
    wide = jnp.concatenate([inv, inv], axis=1)
    rows = jnp.concatenate([scaled[j] for j in range(4)], axis=1)
    glu = (dot(rows, weights[:, 0:256]) * wide).astype(BF16).astype(F32)
    g = (glu[:, 0:128] * jax.nn.sigmoid(glu[:, 128:256])).astype(BF16)
    glued[...] = g
    tail[...] = g[ROWS - 32 :, :]
    gates[:, 128:384] = (dot(rows, weights[:, 256:512]) * wide).astype(BF16)
    gates[:, 0:128] = (dot(rows, weights[:, 512:640]) * inv).astype(BF16)


def conv_kernel(glued, before, weight, conv, squares, kept, padded):
    padded[0:32, :] = before[...].astype(F32)
    padded[32 : 32 + ROWS, :] = glued[...].astype(F32)
    taps = weight[...].astype(F32)
    total = jnp.zeros((ROWS, 128), F32)
    for j in range(WIDTH):
        total += padded[j + 2 : j + 2 + ROWS, :] * taps[j : j + 1, :]
    conv[...] = total
    sums = jnp.sum(jnp.transpose(total * total), axis=0, keepdims=True)
    squares[...] = sums
    kept[...] = sums


def attend(tiles, own, other, slots, queries, maxima, acc, mask=None):
    keys, values, units = [], [], []
    for n, slot in enumerate(slots):
        both = jnp.concatenate([own[slot, 0:256, :], other[slot, 0:256, :]], axis=0)
        keys.append(jnp.concatenate([both, both], axis=1))
        parts = [ref[slot, r : r + 128, :] for ref in (own, other) for r in (256, 384)]
        ones = jnp.ones((ACC - VDIM, 512), BF16)
        values.append(jnp.concatenate([jnp.concatenate(parts, axis=1), ones], axis=0))
        units += [(t, n) for t in tiles]
    ahead = [dot(keys[n], queries[t]) for t, n in units[:DEPTH]]
    for i, (t, n) in enumerate(units):
        scores = ahead.pop(0)
        if i + DEPTH < len(units):
            later, m = units[i + DEPTH]
            ahead.append(dot(keys[m], queries[later]))
        if mask is not None:
            scores = jnp.where(mask, scores, NEG_BIG)
        old = maxima[t]
        new = jnp.maximum(old, jnp.max(scores, axis=0, keepdims=True))
        factor = jnp.exp2(old - new)
        expd = jnp.exp2(scores - new).astype(BF16)
        acc[t] = acc[t] * factor + dot(values[n], expd)
        maxima[t] = new


def attend_before(z, tiles, own, other, queries, maxima, acc):
    def visit(i, carry):
        attend(tiles, own, other, (2 * i, 2 * i + 1), queries, maxima, acc)
        return carry

    lax.fori_loop(0, z // 2, visit, 0)

    @pl.when(lax.rem(z, 2) == 1)
    def _():
        attend(tiles, own, other, (z - 1,), queries, maxima, acc)


def lay_queries(q_refs, queries):
    none = jnp.zeros((64, ROWS), BF16)
    for b, ref in enumerate(q_refs):
        for t in range(4):
            g, m = t // 2, t % 2
            part = ref[g * 128 + m * 64 : g * 128 + m * 64 + 64, :].astype(F32) * LOG2E
            high = part.astype(BF16)
            low = (part - high.astype(F32)).astype(BF16)
            for i, rows in enumerate((high, low)):
                at = i * 128
                queries[b * 4 + t, at + m * 64 : at + m * 64 + 64, :] = rows
                queries[b * 4 + t, at + (1 - m) * 64 : at + (1 - m) * 64 + 64, :] = none


def write_part(out, first, maxima, acc):
    lines = []
    for t in range(4):
        i = first + t
        length = acc[i, VDIM : VDIM + 1, :]
        some = length > 0.0
        safe = jnp.where(some, length, 1.0)
        out[t * VDIM : (t + 1) * VDIM, :] = (acc[i, 0:VDIM, :] * (1.0 / safe)).astype(BF16)
        log = jnp.where(some, maxima[i] + jnp.log2(safe), NEG_BIG)
        for _ in range(3):
            piece = log.astype(BF16).astype(F32)
            lines.append(piece)
            log = log - piece
    lines.append(jnp.zeros((4, ROWS), F32))
    out[4 * VDIM : MSG, :] = jnp.concatenate(lines, axis=0).astype(BF16)


def position():
    s = lax.axis_index("sp")
    return s // 8, lax.rem(s // 2, 4), lax.rem(s, 2)


def start_state(maxima, acc):
    maxima[...] = jnp.full(maxima.shape, NEG_BIG, F32)
    acc[...] = jnp.zeros(acc.shape, F32)


def remote_kernel(q0, q1, q2, own, other, o0, o1, o2, queries, maxima, acc):
    z, y, _ = position()
    lay_queries((q0, q1, q2), queries)
    start_state(maxima, acc)

    attend_before(z, range(12), own, other, queries, maxima, acc)
    for b, by in enumerate(SHIFTS):

        @pl.when(lax.rem(y - by + 4, 4) > y)
        def _(b=b):
            attend(range(4 * b, 4 * b + 4), own, other, (z,), queries, maxima, acc)

    for b, out in enumerate((o0, o1, o2)):
        write_part(out, 4 * b, maxima, acc)


def self_kernel(q0, own, other, out, queries, maxima, acc):
    z, _, c = position()
    lay_queries((q0,), queries)
    start_state(maxima, acc)
    row = lax.broadcasted_iota(jnp.int32, (512, ROWS), 0)
    key_row = jnp.where(row < ROWS, row + c * ROWS, row - c * ROWS)
    query_row = lax.broadcasted_iota(jnp.int32, (512, ROWS), 1) + c * ROWS
    attend(range(4), own, other, (z,), queries, maxima, acc, key_row <= query_row)

    attend_before(z, range(4), own, other, queries, maxima, acc)
    write_part(out, 0, maxima, acc)


def merge_kernel(m0, m1, m2, m3, conv, s0, s1, s2, s3, c_gain, gates, lam, gain, y0, y1, y2, y3, rows):
    x = lax.axis_index("tp")
    total = (s0[...] + s1[...]) + (s2[...] + s3[...])
    inv = lax.rsqrt(total / CONV + EPSILON)
    inv = jnp.transpose(jnp.broadcast_to(inv, (128, ROWS)))
    normed = conv[...] * inv * c_gain[...]
    y_conv = (jax.nn.silu(normed) * jax.nn.silu(gates[:, 0:128].astype(F32))).astype(BF16)
    for j in range(4):
        rows[j, :, 0:128] = y_conv[64 * j : 64 * j + 64, :]
    logs = []
    for ref in (m0, m1, m2, m3):
        stats = ref[4 * VDIM : MSG, :].astype(F32)
        logs.append([(stats[3 * t : 3 * t + 1] + stats[3 * t + 1 : 3 * t + 2]) + stats[3 * t + 2 : 3 * t + 3] for t in range(4)])
    for g in range(2):
        maps = []
        for m in range(2):
            t = 2 * g + m
            top = functools.reduce(jnp.maximum, [l[t] for l in logs])
            weights = [jnp.exp2(l[t] - top) for l in logs]
            norm = 1.0 / functools.reduce(jnp.add, weights)
            part = [r[t * VDIM : (t + 1) * VDIM, :].astype(F32) * (w * norm) for r, w in zip((m0, m1, m2, m3), weights)]
            maps.append((part[0] + part[1]) + (part[2] + part[3]))
        o = maps[0] - lam[g] * maps[1]
        o = o * lax.rsqrt(jnp.mean(o * o, axis=0, keepdims=True) + EPSILON)
        o = jnp.transpose(o) * gain[...] * HEAD_SCALE
        gate = gates[:, 128 + g * 128 : 256 + g * 128].astype(F32)
        o = (o * jax.nn.silu(gate)).astype(BF16)
        for j in range(4):
            rows[j, :, 128 + g * 128 : 256 + g * 128] = o[64 * j : 64 * j + 64, :]
    for ref, by in zip((y0, y1, y2, y3), (0,) + SHIFTS):
        ref[...] = rows[lax.rem(x + by + 4, 4)]


def output_kernel(y0, y1, y2, y3, w_conv, w_attn, a1, a2, a3, b1, b2, b3, out):
    c = lax.rem(lax.axis_index("sp"), 2)
    y = y0[...]
    theirs = jnp.concatenate([y1[...], y2[...], y3[...]], axis=1)
    for half, refs in ((c, (a1, a2, a3)), (1 - c, (b1, b2, b3))):
        at = pl.ds(pl.multiple_of(half * 1024, 1024), 1024)
        mine = dot(y[:, 0:128], w_conv[:, at]) + dot(y[:, 128:384], w_attn[:, at])
        weights = jnp.concatenate([r[...] for r in refs], axis=0)
        out[:, at] = (mine + dot(theirs, weights)).astype(BF16)


def shape(dims, kind=BF16):
    return jax.ShapeDtypeStruct(dims, kind)


def sent(dims, kind=BF16):
    return pltpu.MemorySpace.HBM(dims, kind)


def local(
    tokens,
    in_gain,
    w_glu_value,
    w_glu_gate,
    w_query,
    w_key,
    w_value,
    w_gate_conv,
    w_gate_attn,
    conv_weight,
    conv_gain,
    lam,
    head_gain,
    out_conv,
    out_attn,
):
    c = lax.rem(lax.axis_index("sp"), 2)
    half = lax.dynamic_slice_in_dim(jnp.concatenate([out_conv, out_attn], axis=0), c * 1024, 1024, 1)
    pieces = [tokens] + [tp_shift(tokens, by) for by in SHIFTS]
    gain = in_gain.astype(F32).reshape(4, 512)
    first = jnp.concatenate([w_query, w_key, w_value], axis=1)
    second = jnp.concatenate([w_glu_value, w_glu_gate, w_gate_attn, w_gate_conv], axis=1)
    gain, first, second, half = lax.optimization_barrier((gain, first, second, half))
    qt, kv, scaled, inv = pl.pallas_call(
        project_kernel,
        out_shape=[sent((256, ROWS)), sent((8, 512, 128)), sent((4, ROWS, 512)), sent((ROWS, 128), F32)],
        in_specs=[VM] * 6,
        out_specs=[OUT] * 4,
        compiler_params=SMALL,
        name="project",
    )(*pieces, gain, first)

    groups = [[z * 8 + r for z in range(8)] for r in range(8)]
    gathered = lax.all_to_all(kv, "sp", 0, 0, tiled=True, axis_index_groups=groups)
    q_blocks = [y_shift(qt, by) for by in SHIFTS]
    weights = [tp_shift(half, by) for by in SHIFTS]

    glued, tail, gates = pl.pallas_call(
        rest_kernel,
        out_shape=[shape((ROWS, 128)), sent((32, 128)), shape((ROWS, 384))],
        in_specs=[VM] * 3,
        out_specs=[VM, OUT, VM],
        compiler_params=SMALL,
        name="rest",
    )(scaled, inv, second)
    before = lax.ppermute(tail, "sp", [(i, i + 1) for i in range(63)])
    conv, squares, kept = pl.pallas_call(
        conv_kernel,
        out_shape=[shape((ROWS, 128), F32), sent((1, ROWS), F32), shape((1, ROWS), F32)],
        in_specs=[VM] * 3,
        out_specs=[VM, OUT, VM],
        scratch_shapes=[pltpu.VMEM((32 + ROWS, 128), F32)],
        compiler_params=SMALL,
        name="conv",
    )(glued, before, conv_weight)
    sums = [kept] + [tp_shift(squares, by) for by in SHIFTS]

    swapped = core_swap(gathered)

    def scratch(tiles):
        return [
            pltpu.VMEM((tiles, 256, ROWS), BF16),
            pltpu.VMEM((tiles, 1, ROWS), F32),
            pltpu.VMEM((tiles, ACC, ROWS), F32),
        ]

    parts = pl.pallas_call(
        remote_kernel,
        out_shape=[sent((MSG, ROWS))] * 3,
        in_specs=[VM] * 5,
        out_specs=[OUT] * 3,
        scratch_shapes=scratch(12),
        compiler_params=BIG,
        name="remote",
    )(*q_blocks, gathered, swapped)
    back = [y_shift(part, -by) for part, by in zip(parts, SHIFTS)]
    parts, qt, weights = lax.optimization_barrier((parts, qt, weights))
    weights_s = [core_swap(w) for w in weights]
    part = pl.pallas_call(
        self_kernel,
        out_shape=shape((MSG, ROWS)),
        in_specs=[VM] * 3,
        out_specs=VM,
        scratch_shapes=scratch(4),
        compiler_params=BIG,
        name="self",
    )(qt, gathered, swapped)

    rows = pl.pallas_call(
        merge_kernel,
        out_shape=[shape((64, 384))] + [sent((64, 384))] * 3,
        in_specs=[VM] * 11 + [SM, VM],
        out_specs=[VM] + [OUT] * 3,
        scratch_shapes=[pltpu.VMEM((4, 64, 384), BF16)],
        compiler_params=SMALL,
        name="merge",
    )(part, *back, conv, *sums, conv_gain.reshape(1, 128), gates, lam, head_gain.reshape(1, 128))
    rows = [rows[0]] + [tp_shift(r, by) for r, by in zip(rows[1:], SHIFTS)]
    return pl.pallas_call(
        output_kernel,
        out_shape=shape((64, D)),
        in_specs=[VM] * 12,
        out_specs=VM,
        compiler_params=BIG,
        name="output",
    )(*rows, out_conv, out_attn, *weights, *weights_s)


def solution(mesh):
    in_specs = (
        P("sp", "tp"),
        P(),
        P(None, "tp"),
        P(None, "tp"),
        P(None, "tp"),
        P(None, "tp"),
        P(None, "tp"),
        P(None, "tp"),
        P(None, "tp"),
        P(None, "tp"),
        P("tp"),
        P("tp"),
        P(),
        P("tp", None),
        P("tp", None),
    )
    out_specs = P(("sp", "tp"), None)

    return jax.shard_map(local, mesh=mesh, in_specs=in_specs, out_specs=out_specs, check_vma=False)
```

```python
import functools

import jax
import jax.numpy as jnp
from jax import lax
from jax.experimental import pallas as pl
from jax.experimental.pallas import tpu as pltpu
from jax.sharding import PartitionSpec as P


D = 2048
CONV = 512
QK = 64
VDIM = 128
WIDTH = 31
ROWS = 256
ACC = VDIM + 16
MSG = 4 * VDIM + 16

EPSILON = 1e-06
NEG_BIG = -1e30
HEAD_SCALE = 0.8


F32 = jnp.float32
BF16 = jnp.bfloat16
VM = pl.BlockSpec(memory_space=pltpu.VMEM)
OUT = pl.BlockSpec()
SM = pl.BlockSpec(memory_space=pltpu.SMEM)
ANY = pl.BlockSpec(memory_space=pltpu.MemorySpace.HBM)
BIG = pltpu.CompilerParams(vmem_limit_bytes=16 * 1024 * 1024)
SMALL = pltpu.CompilerParams(vmem_limit_bytes=8 * 1024 * 1024)
SHIFTS = (1, -1, 2)
DEPTH = 3
LOG2E = 1.4426950408889634


def place(s):
    return s // 8, (s // 2) % 4, s % 2


def along_sp(x, move):
    pairs = []
    for s in range(64):
        z, y, c = place(s)
        z, y, c = move(z, y, c)
        pairs.append((s, z * 8 + y * 2 + c))
    return lax.ppermute(x, "sp", pairs)


def y_shift(x, by):
    return along_sp(x, lambda z, y, c: (z, (y + by) % 4, c))


def core_swap(x):
    return along_sp(x, lambda z, y, c: (z, y, 1 - c))


def tp_shift(x, by):
    return lax.ppermute(x, "tp", [(i, (i + by) % 4) for i in range(4)])


def dot(a, b):
    return jnp.dot(a, b, preferred_element_type=F32)


def project_kernel(t0, t1, t2, t3, gain, weights, qt, kv, alone, scaled, inv_out):
    x = lax.axis_index("tp")
    squares = jnp.zeros((ROWS, 128), F32)
    for ref, by in zip((t0, t1, t2, t3), (0,) + SHIFTS):
        j = lax.rem(x - by + 4, 4)
        wide = ref[...].astype(F32)
        scaled[j] = (wide * gain[pl.ds(j, 1), :]).astype(BF16)
        sq = wide * wide
        squares += (sq[:, 0:128] + sq[:, 128:256]) + (sq[:, 256:384] + sq[:, 384:512])
    inv = lax.rsqrt(jnp.sum(squares, axis=1, keepdims=True) / D + EPSILON)
    inv_out[...] = jnp.broadcast_to(inv, (ROWS, 128))
    rows = jnp.concatenate([scaled[j] for j in range(4)], axis=1)
    both = dot(rows, weights[:, 256:512]) * inv
    k = both[:, 0:128].astype(BF16)
    vt = jnp.transpose(both[:, 128:256]).astype(BF16)
    for ref, z in [(kv, z) for z in range(8)] + [(alone, 0)]:
        ref[z, 0:256, :] = k
        ref[z, 256:384, :] = vt[:, 0:128]
        ref[z, 384:512, :] = vt[:, 128:256]
    q = dot(rows, weights[:, 0:256]) * inv
    qt[...] = jnp.transpose(q * (QK ** -0.5)).astype(BF16)


def rest_kernel(scaled, inv_in, weights, glued, tail, gates):
    inv = inv_in[...]
    wide = jnp.concatenate([inv, inv], axis=1)
    rows = jnp.concatenate([scaled[j] for j in range(4)], axis=1)
    glu = (dot(rows, weights[:, 0:256]) * wide).astype(BF16).astype(F32)
    g = (glu[:, 0:128] * jax.nn.sigmoid(glu[:, 128:256])).astype(BF16)
    glued[...] = g
    tail[...] = g[ROWS - 32 :, :]
    gates[:, 128:384] = (dot(rows, weights[:, 256:512]) * wide).astype(BF16)
    gates[:, 0:128] = (dot(rows, weights[:, 512:640]) * inv).astype(BF16)


def conv_kernel(glued, before, weight, conv, squares, kept, padded):
    padded[0:32, :] = before[...].astype(F32)
    padded[32 : 32 + ROWS, :] = glued[...].astype(F32)
    taps = weight[...].astype(F32)
    total = jnp.zeros((ROWS, 128), F32)
    for j in range(WIDTH):
        total += padded[j + 2 : j + 2 + ROWS, :] * taps[j : j + 1, :]
    conv[...] = total
    sums = jnp.sum(jnp.transpose(total * total), axis=0, keepdims=True)
    squares[...] = sums
    kept[...] = sums


def attend(tiles, own, other, slots, queries, maxima, acc, mask=None):
    keys, values, units = [], [], []
    for n, slot in enumerate(slots):
        both = jnp.concatenate([own[slot, 0:256, :], other[slot, 0:256, :]], axis=0)
        keys.append(jnp.concatenate([both, both], axis=1))
        parts = [ref[slot, r : r + 128, :] for ref in (own, other) for r in (256, 384)]
        ones = jnp.ones((ACC - VDIM, 512), BF16)
        values.append(jnp.concatenate([jnp.concatenate(parts, axis=1), ones], axis=0))
        units += [(t, n) for t in tiles]
    ahead = [dot(keys[n], queries[t]) for t, n in units[:DEPTH]]
    for i, (t, n) in enumerate(units):
        scores = ahead.pop(0)
        if i + DEPTH < len(units):
            later, m = units[i + DEPTH]
            ahead.append(dot(keys[m], queries[later]))
        if mask is not None:
            scores = jnp.where(mask, scores, NEG_BIG)
        old = maxima[t]
        new = jnp.maximum(old, jnp.max(scores, axis=0, keepdims=True))
        factor = jnp.exp2(old - new)
        expd = jnp.exp2(scores - new).astype(BF16)
        acc[t] = acc[t] * factor + dot(values[n], expd)
        maxima[t] = new


def attend_before(z, tiles, own, other, queries, maxima, acc):
    def visit(i, carry):
        attend(tiles, own, other, (2 * i, 2 * i + 1), queries, maxima, acc)
        return carry

    lax.fori_loop(0, z // 2, visit, 0)

    @pl.when(lax.rem(z, 2) == 1)
    def _():
        attend(tiles, own, other, (z - 1,), queries, maxima, acc)


def lay_queries(q_refs, queries):
    none = jnp.zeros((64, ROWS), BF16)
    for b, ref in enumerate(q_refs):
        for t in range(4):
            g, m = t // 2, t % 2
            part = ref[g * 128 + m * 64 : g * 128 + m * 64 + 64, :].astype(F32) * LOG2E
            high = part.astype(BF16)
            low = (part - high.astype(F32)).astype(BF16)
            for i, rows in enumerate((high, low)):
                at = i * 128
                queries[b * 4 + t, at + m * 64 : at + m * 64 + 64, :] = rows
                queries[b * 4 + t, at + (1 - m) * 64 : at + (1 - m) * 64 + 64, :] = none


def write_part(out, first, maxima, acc):
    lines = []
    for t in range(4):
        i = first + t
        length = acc[i, VDIM : VDIM + 1, :]
        some = length > 0.0
        safe = jnp.where(some, length, 1.0)
        out[t * VDIM : (t + 1) * VDIM, :] = (acc[i, 0:VDIM, :] * (1.0 / safe)).astype(BF16)
        log = jnp.where(some, maxima[i] + jnp.log2(safe), NEG_BIG)
        for _ in range(3):
            piece = log.astype(BF16).astype(F32)
            lines.append(piece)
            log = log - piece
    lines.append(jnp.zeros((4, ROWS), F32))
    out[4 * VDIM : MSG, :] = jnp.concatenate(lines, axis=0).astype(BF16)


def position():
    s = lax.axis_index("sp")
    return s // 8, lax.rem(s // 2, 4), lax.rem(s, 2)


def start_state(maxima, acc):
    maxima[...] = jnp.full(maxima.shape, NEG_BIG, F32)
    acc[...] = jnp.zeros(acc.shape, F32)


def near_kernel(q0, q1, q2, q3, own, other, far_max, far_acc, self_max, self_acc, far_queries, self_queries):
    _, y, c = position()
    lay_queries((q0, q1, q2), far_queries)
    lay_queries((q3,), self_queries)
    start_state(far_max, far_acc)
    start_state(self_max, self_acc)
    row = lax.broadcasted_iota(jnp.int32, (512, ROWS), 0)
    key_row = jnp.where(row < ROWS, row + c * ROWS, row - c * ROWS)
    query_row = lax.broadcasted_iota(jnp.int32, (512, ROWS), 1) + c * ROWS
    attend(range(4), own, other, (0,), self_queries, self_max, self_acc, key_row <= query_row)
    for b, by in enumerate(SHIFTS):

        @pl.when(lax.rem(y - by + 4, 4) > y)
        def _(b=b):
            attend(range(4 * b, 4 * b + 4), own, other, (0,), far_queries, far_max, far_acc)


def remote_kernel(q0, q1, q2, own, other, max_in, acc_in, o0, o1, o2, queries, maxima, acc):
    z, _, _ = position()
    lay_queries((q0, q1, q2), queries)
    maxima[...] = max_in[...]
    acc[...] = acc_in[...]
    attend_before(z, range(12), own, other, queries, maxima, acc)
    for b, out in enumerate((o0, o1, o2)):
        write_part(out, 4 * b, maxima, acc)


def self_kernel(q0, own, other, max_in, acc_in, out, queries, maxima, acc):
    z, _, _ = position()
    lay_queries((q0,), queries)
    maxima[...] = max_in[...]
    acc[...] = acc_in[...]
    attend_before(z, range(4), own, other, queries, maxima, acc)
    write_part(out, 0, maxima, acc)


def merge_kernel(m0, m1, m2, m3, conv, s0, s1, s2, s3, c_gain, gates, lam, gain, y0, y1, y2, y3, rows):
    x = lax.axis_index("tp")
    total = (s0[...] + s1[...]) + (s2[...] + s3[...])
    inv = lax.rsqrt(total / CONV + EPSILON)
    inv = jnp.transpose(jnp.broadcast_to(inv, (128, ROWS)))
    normed = conv[...] * inv * c_gain[...]
    y_conv = (jax.nn.silu(normed) * jax.nn.silu(gates[:, 0:128].astype(F32))).astype(BF16)
    for j in range(4):
        rows[j, :, 0:128] = y_conv[64 * j : 64 * j + 64, :]
    logs = []
    for ref in (m0, m1, m2, m3):
        stats = ref[4 * VDIM : MSG, :].astype(F32)
        logs.append([(stats[3 * t : 3 * t + 1] + stats[3 * t + 1 : 3 * t + 2]) + stats[3 * t + 2 : 3 * t + 3] for t in range(4)])
    for g in range(2):
        maps = []
        for m in range(2):
            t = 2 * g + m
            top = functools.reduce(jnp.maximum, [l[t] for l in logs])
            weights = [jnp.exp2(l[t] - top) for l in logs]
            norm = 1.0 / functools.reduce(jnp.add, weights)
            part = [r[t * VDIM : (t + 1) * VDIM, :].astype(F32) * (w * norm) for r, w in zip((m0, m1, m2, m3), weights)]
            maps.append((part[0] + part[1]) + (part[2] + part[3]))
        o = maps[0] - lam[g] * maps[1]
        o = o * lax.rsqrt(jnp.mean(o * o, axis=0, keepdims=True) + EPSILON)
        o = jnp.transpose(o) * gain[...] * HEAD_SCALE
        gate = gates[:, 128 + g * 128 : 256 + g * 128].astype(F32)
        o = (o * jax.nn.silu(gate)).astype(BF16)
        for j in range(4):
            rows[j, :, 128 + g * 128 : 256 + g * 128] = o[64 * j : 64 * j + 64, :]
    for ref, by in zip((y0, y1, y2, y3), (0,) + SHIFTS):
        ref[...] = rows[lax.rem(x + by + 4, 4)]


def output_kernel(y0, y1, y2, y3, w_conv, w_attn, a1, a2, a3, b1, b2, b3, out):
    c = lax.rem(lax.axis_index("sp"), 2)
    y = y0[...]
    theirs = jnp.concatenate([y1[...], y2[...], y3[...]], axis=1)
    for half, refs in ((c, (a1, a2, a3)), (1 - c, (b1, b2, b3))):
        at = pl.ds(pl.multiple_of(half * 1024, 1024), 1024)
        mine = dot(y[:, 0:128], w_conv[:, at]) + dot(y[:, 128:384], w_attn[:, at])
        weights = jnp.concatenate([r[...] for r in refs], axis=0)
        out[:, at] = (mine + dot(theirs, weights)).astype(BF16)


def shape(dims, kind=BF16):
    return jax.ShapeDtypeStruct(dims, kind)


def sent(dims, kind=BF16):
    return pltpu.MemorySpace.HBM(dims, kind)


def local(
    tokens,
    in_gain,
    w_glu_value,
    w_glu_gate,
    w_query,
    w_key,
    w_value,
    w_gate_conv,
    w_gate_attn,
    conv_weight,
    conv_gain,
    lam,
    head_gain,
    out_conv,
    out_attn,
):
    c = lax.rem(lax.axis_index("sp"), 2)
    half = lax.dynamic_slice_in_dim(jnp.concatenate([out_conv, out_attn], axis=0), c * 1024, 1024, 1)
    pieces = [tokens] + [tp_shift(tokens, by) for by in SHIFTS]
    gain = in_gain.astype(F32).reshape(4, 512)
    first = jnp.concatenate([w_query, w_key, w_value], axis=1)
    second = jnp.concatenate([w_glu_value, w_glu_gate, w_gate_attn, w_gate_conv], axis=1)
    gain, first, second, half = lax.optimization_barrier((gain, first, second, half))
    qt, kv, alone, scaled, inv = pl.pallas_call(
        project_kernel,
        out_shape=[sent((256, ROWS)), sent((8, 512, 128)), sent((1, 512, 128)), sent((4, ROWS, 512)), sent((ROWS, 128), F32)],
        in_specs=[VM] * 6,
        out_specs=[OUT] * 5,
        compiler_params=SMALL,
        name="project",
    )(*pieces, gain, first)

    groups = [[z * 8 + r for z in range(8)] for r in range(8)]
    gathered = lax.all_to_all(kv, "sp", 0, 0, tiled=True, axis_index_groups=groups)
    q_blocks = [y_shift(qt, by) for by in SHIFTS]
    weights = [tp_shift(half, by) for by in SHIFTS]

    glued, tail, gates = pl.pallas_call(
        rest_kernel,
        out_shape=[shape((ROWS, 128)), sent((32, 128)), shape((ROWS, 384))],
        in_specs=[VM] * 3,
        out_specs=[VM, OUT, VM],
        compiler_params=SMALL,
        name="rest",
    )(scaled, inv, second)
    before = lax.ppermute(tail, "sp", [(i, i + 1) for i in range(63)])
    conv, squares, kept = pl.pallas_call(
        conv_kernel,
        out_shape=[shape((ROWS, 128), F32), sent((1, ROWS), F32), shape((1, ROWS), F32)],
        in_specs=[VM] * 3,
        out_specs=[VM, OUT, VM],
        scratch_shapes=[pltpu.VMEM((32 + ROWS, 128), F32)],
        compiler_params=SMALL,
        name="conv",
    )(glued, before, conv_weight)
    sums = [kept] + [tp_shift(squares, by) for by in SHIFTS]

    swapped = core_swap(gathered)

    def scratch(tiles):
        return [
            pltpu.VMEM((tiles, 256, ROWS), BF16),
            pltpu.VMEM((tiles, 1, ROWS), F32),
            pltpu.VMEM((tiles, ACC, ROWS), F32),
        ]

    far_max, far_acc, self_max, self_acc = pl.pallas_call(
        near_kernel,
        out_shape=[shape((n, r, ROWS), F32) for n in (12, 4) for r in (1, ACC)],
        in_specs=[VM] * 6,
        out_specs=[VM] * 4,
        scratch_shapes=[pltpu.VMEM((12, 256, ROWS), BF16), pltpu.VMEM((4, 256, ROWS), BF16)],
        compiler_params=BIG,
        name="near",
    )(*q_blocks, qt, alone, core_swap(alone))

    parts = pl.pallas_call(
        remote_kernel,
        out_shape=[sent((MSG, ROWS))] * 3,
        in_specs=[VM] * 7,
        out_specs=[OUT] * 3,
        scratch_shapes=scratch(12),
        compiler_params=BIG,
        name="remote",
    )(*q_blocks, gathered, swapped, far_max, far_acc)
    back = [y_shift(part, -by) for part, by in zip(parts, SHIFTS)]
    parts, qt, weights = lax.optimization_barrier((parts, qt, weights))
    weights_s = [core_swap(w) for w in weights]
    part = pl.pallas_call(
        self_kernel,
        out_shape=shape((MSG, ROWS)),
        in_specs=[VM] * 5,
        out_specs=VM,
        scratch_shapes=scratch(4),
        compiler_params=BIG,
        name="self",
    )(qt, gathered, swapped, self_max, self_acc)

    rows = pl.pallas_call(
        merge_kernel,
        out_shape=[shape((64, 384))] + [sent((64, 384))] * 3,
        in_specs=[VM] * 11 + [SM, VM],
        out_specs=[VM] + [OUT] * 3,
        scratch_shapes=[pltpu.VMEM((4, 64, 384), BF16)],
        compiler_params=SMALL,
        name="merge",
    )(part, *back, conv, *sums, conv_gain.reshape(1, 128), gates, lam, head_gain.reshape(1, 128))
    rows = [rows[0]] + [tp_shift(r, by) for r, by in zip(rows[1:], SHIFTS)]
    return pl.pallas_call(
        output_kernel,
        out_shape=shape((64, D)),
        in_specs=[VM] * 12,
        out_specs=VM,
        compiler_params=BIG,
        name="output",
    )(*rows, out_conv, out_attn, *weights, *weights_s)


def solution(mesh):
    in_specs = (
        P("sp", "tp"),
        P(),
        P(None, "tp"),
        P(None, "tp"),
        P(None, "tp"),
        P(None, "tp"),
        P(None, "tp"),
        P(None, "tp"),
        P(None, "tp"),
        P(None, "tp"),
        P("tp"),
        P("tp"),
        P(),
        P("tp", None),
        P("tp", None),
    )
    out_specs = P(("sp", "tp"), None)

    return jax.shard_map(local, mesh=mesh, in_specs=in_specs, out_specs=out_specs, check_vma=False)
```
